256 devices in a mesh: ep: 64 (over z, y, core), tp: 4 (over x).
Axes of the slice: x: 4, y: 4, z: 8, core: 2. Of those that a mesh axis runs over, the one named last changes fastest.
Arguments:
- tokens: bfloat16 [2048, 2048], P('ep', 'tp'), may hold values from -33 to 33
- previous: bfloat16 [2048, 2048], P('ep', 'tp'), may hold values from -6 to 6
- first_norm_gain: float32 [2048], replicated, may hold values from 0.1 to 1.9
- token_shift_share: float32 [5, 2048], replicated, may hold values from 0 to 1
- receptance_weight: bfloat16 [2048, 1024], P(None, 'tp'), may hold values from -0.125 to 0.125
- key_weight: bfloat16 [2048, 1024], P(None, 'tp'), may hold values from -0.125 to 0.125
- value_weight: bfloat16 [2048, 1024], P(None, 'tp'), may hold values from -0.125 to 0.125
- decay_down_map: bfloat16 [2048, 128], replicated, may hold values from -0.125 to 0.125
- decay_up_map: bfloat16 [128, 1024], replicated, may hold values from -0.5 to 0.5
- decay_offset: float32 [1024], P('tp'), may hold values from -4 to 1
- strength_down_map: bfloat16 [2048, 128], replicated, may hold values from -0.125 to 0.125
- strength_up_map: bfloat16 [128, 1024], replicated, may hold values from -0.5 to 0.5
- removal_key_scale: float32 [1024], P('tp'), may hold values from 0.3 to 3
- key_damping: float32 [1024], P('tp'), may hold values from 0.1 to 1.9
- self_term_weight: float32 [16, 64], P('tp'), may hold values from -0.6 to 0.6
- head_norm_gain: float32 [1024], P('tp'), may hold values from 0.1 to 1.9
- output_weight: bfloat16 [1024, 2048], P('tp'), may hold values from -0.1875 to 0.1875
- state: float32 [2048, 16, 64, 64], P('ep', 'tp'), may hold values from -6 to 6
- second_norm_gain: float32 [2048], replicated, may hold values from 0.1 to 1.9
- routes: int32 [2048, 4], P('ep'), may hold values from 0 to 63, all different within a row; in each aligned block of 32 rows (0 to 31, 32 to 63, ...) at most 3 rows name the same one
- chosen_expert_weight: float32 [2048, 4], P('ep'), may hold values from 0.1 to 1
- expert_gate_weight: bfloat16 [64, 2048, 1024], P('ep', None, 'tp'), may hold values from -0.5 to 0.5
- expert_up_weight: bfloat16 [64, 2048, 1024], P('ep', None, 'tp'), may hold values from -0.5 to 0.5
- expert_down_weight: bfloat16 [64, 1024, 2048], P('ep', 'tp'), may hold values from -0.046875 to 0.046875
Outputs:
- layer_out: bfloat16 [2048, 2048], P('ep', 'tp')
- new_state: float32 [2048, 16, 64, 64], P('ep', 'tp')
The draws below stay inside these ranges and needn't reach their ends.
Inputs may be any that keep to these rules, and one draw needn't show every extreme that they name: `routes`: each row names 4 different experts. Among the rows of one index of ep no expert is named by more than 3 rows, and in every draw some expert is named by exactly 3 rows of some index of ep.
All inputs are finite; a program needn't handle non-finite values.
Results may differ from the reference program's by a relative error of at most 0.015.
Values may be sent and summed in bfloat16 or wider, within the bound.
No kernel may reach another device: no remote copies, remote signals or barrier semaphores. Data moves between devices by JAX's collectives and lax.ppermute only.
A program may use at most 64 MiB of HBM per device.

```python
import math
import jax
import jax.numpy as jnp
import numpy as np
from jax import lax

D = 2048
HEAD_TOTAL = 16
HEAD_WIDTH = 64
DECAY_RANK = 128
ALPHA_RANK = 128
FF = 1024
TOP_K = 4
SEQ_DEV = 32
SEQS = 2048
EXPERTS = 64
CAP = 3
N_EP = 64
N_TP = 4


def draw_tokens(key, part):
    row_key = jax.random.fold_in(key, 11)
    col_key = jax.random.fold_in(key, 12)
    base_key = jax.random.fold_in(key, 13)
    row_scales = jnp.exp(jax.random.uniform(row_key, (SEQS, 1), jnp.float32, -0.69, 0.69))
    ramp = jnp.exp((jnp.arange(D, dtype=jnp.float32) / D - 0.5) * 1.0986)
    col_scales = jnp.exp(jax.random.uniform(col_key, (1, D), jnp.float32, -1.15, 1.15)) * ramp[None, :]
    base = jnp.clip(jax.random.normal(base_key, (SEQS, D), jnp.float32), -3.0, 3.0)
    return (base * row_scales * col_scales).astype(jnp.bfloat16)


def block_levels(stream_key, extent, pieces, low, top_value):
    loudness, own = 1.0, jax.random.fold_in(stream_key, 6)
    for axis_at, shards_of in pieces:
        steps = jnp.exp(jax.random.uniform(jax.random.fold_in(own, axis_at), (shards_of,), jnp.float32, low / len(pieces), top_value / len(pieces)))
        loudness = loudness * jnp.repeat(steps, extent[axis_at] // shards_of).reshape([-1 if axis == axis_at else 1 for axis in range(len(extent))])
    return loudness


def assign_block(key, own, number, rows, count, top, reach, skew):
    order = jax.random.permutation(key, count)
    crowded, usual = portions_of(count, rows * top, reach, skew, True), portions_of(count, rows * top, reach, skew, False)
    places = jnp.arange(count)

    def named(tallies, turn):
        used = int((tallies > 0).sum())
        fixed = max(1, used // 4)
        passed = fixed + (places - fixed + turn * (used - fixed)) % max(1, count - fixed)
        return jnp.zeros((count,), jnp.int32).at[order[jnp.where(places < fixed, places, passed)]].set(jnp.asarray(tallies, jnp.int32))

    tallies = jnp.where(number % 4 == 0, named(crowded, number // 4), named(usual, number - number // 4 - 1))
    mixed = jax.random.permutation(jax.random.fold_in(own, 3), count)
    giver, sink = mixed[0:count // 2 * 2:2], mixed[1:count // 2 * 2:2]
    room = jnp.minimum(tallies[giver] - 1, reach - tallies[sink]) // 2
    room = jnp.where((giver == order[0]) | (sink == order[0]) | (tallies[sink] == 0), 0, jnp.maximum(room, 0))
    passed = jax.random.randint(jax.random.fold_in(own, 4), (count // 2,), 0, 1 << 20) % (room + 1)
    tallies = tallies.at[giver].add(-passed).at[sink].add(passed)
    labels = jnp.searchsorted(jnp.cumsum(tallies), jnp.arange(rows * top), side="right").astype(jnp.int32)
    table = labels.reshape(top, rows).T
    table = table[jax.random.permutation(jax.random.fold_in(own, 1), rows)]
    turn = jax.random.randint(jax.random.fold_in(own, 2), (rows, 1), 0, top)
    return jnp.take_along_axis(table, (jnp.arange(top)[None, :] + turn) % top, axis=1)


def portions_of(number_of, total, reach, slope, full):
    weights = [(1 << 20) // math.isqrt(grade ** slope) + 1 for grade in range(1, number_of + 1)]
    largest = reach if full else min(reach, max(-(-total // number_of), total * weights[0] // sum(weights)))
    least = 1 if total - largest >= number_of - 1 else 0
    holding, rest = [largest] + [least] * (number_of - 1), total - largest - least * (number_of - 1)
    while rest > 0:
        free = [i for i in range(1, number_of) if holding[i] < largest] or [i for i in range(1, number_of) if holding[i] < reach]
        mass, left = sum([weights[i] for i in free]), rest
        for i in free:
            extra = min(reach - holding[i], max(1, left * weights[i] // mass), rest)
            holding[i] = holding[i] + extra
            rest = rest - extra
    return np.array(holding)


def centred(key, shape, deviation, most, cuts=(), kind=jnp.bfloat16):
    result = jax.random.normal(key, shape, jnp.float32) * deviation
    if len(cuts) > 0:
        result = block_levels(key, shape, cuts, -0.22, 0.18) * result
    return jnp.clip(result, min=-most, max=most).astype(kind)


def setup_inputs(seed: int = 0) -> dict:
    key_list = jax.random.split(jax.random.key(seed), 25)
    tokens = draw_tokens(jax.random.fold_in(key_list[24], 71), 0)
    previous = centred(key_list[1], (SEQS, D), 1.0, 6.0, ((0, 64), (1, 4)))
    first_norm_gain = jnp.clip(1.0 + 0.18 * jax.random.normal(key_list[2], (D,), jnp.float32), 0.1, 1.9)
    token_shift_share = jnp.clip(jax.random.uniform(key_list[3], (5, D), jnp.float32, 0.0, 1.0), 0.0, 1.0)
    receptance_weight = centred(key_list[4], (D, HEAD_TOTAL * HEAD_WIDTH), D ** -0.5, 0.125, ((1, 4),))
    key_weight = centred(key_list[5], (D, HEAD_TOTAL * HEAD_WIDTH), D ** -0.5, 0.125, ((1, 4),))
    value_weight = centred(key_list[6], (D, HEAD_TOTAL * HEAD_WIDTH), D ** -0.5, 0.125, ((1, 4),))
    decay_down_map = centred(key_list[7], (D, DECAY_RANK), D ** -0.5, 0.125)
    decay_up_map = centred(key_list[8], (DECAY_RANK, HEAD_TOTAL * HEAD_WIDTH), DECAY_RANK ** -0.5, 0.5)
    decay_offset = jnp.clip(-4.0 + 5.0 * jax.random.uniform(key_list[9], (HEAD_TOTAL * HEAD_WIDTH,), jnp.float32) ** block_levels(key_list[9], (HEAD_TOTAL * HEAD_WIDTH,), ((0, 4),), -0.2, 0.2), -4.0, 1.0)
    strength_down_map = centred(key_list[10], (D, ALPHA_RANK), D ** -0.5, 0.125)
    strength_up_map = centred(key_list[11], (ALPHA_RANK, HEAD_TOTAL * HEAD_WIDTH), ALPHA_RANK ** -0.5, 0.5)
    removal_key_scale = jnp.clip(jnp.exp(math.log(3.0) - 2.3025851 * jax.random.uniform(key_list[12], (HEAD_TOTAL * HEAD_WIDTH,), jnp.float32) ** block_levels(key_list[12], (HEAD_TOTAL * HEAD_WIDTH,), ((0, 4),), -0.2, 0.2)), 0.3, 3.0)
    key_damping = jnp.clip(1.0 + 0.18 * jax.random.normal(key_list[13], (HEAD_TOTAL * HEAD_WIDTH,), jnp.float32), 0.1, 1.9)
    self_term_weight = centred(key_list[14], (HEAD_TOTAL, HEAD_WIDTH), 0.1, 0.6, ((0, 4),), jnp.float32)
    head_norm_gain = jnp.clip(1.0 + 0.18 * jax.random.normal(key_list[15], (HEAD_TOTAL * HEAD_WIDTH,), jnp.float32), 0.1, 1.9)
    output_weight = centred(key_list[16], (HEAD_TOTAL * HEAD_WIDTH, D), (HEAD_TOTAL * HEAD_WIDTH) ** -0.5, 0.1875, ((0, 4),))
    state = centred(key_list[17], (SEQS, HEAD_TOTAL, HEAD_WIDTH, HEAD_WIDTH), 1.0, 6.0, ((0, 64), (1, 4)), jnp.float32)
    second_norm_gain = jnp.clip(1.0 + 0.18 * jax.random.normal(key_list[18], (D,), jnp.float32), 0.1, 1.9)
    routes_keys = jax.random.split(jax.random.fold_in(key_list[19], 1), SEQS // SEQ_DEV)
    routes_turns = jax.random.permutation(jax.random.fold_in(key_list[19], 3), SEQS // SEQ_DEV)
    routes = jax.vmap(lambda own, number: assign_block(jax.random.fold_in(key_list[19], 2), own, number, SEQ_DEV, EXPERTS, TOP_K, CAP, 2))(routes_keys, routes_turns).reshape((SEQS, TOP_K))
    chosen_expert_weight = jnp.clip(jnp.exp(math.log(1.0) - 2.3025851 * jax.random.uniform(key_list[20], (SEQS, TOP_K), jnp.float32) ** block_levels(key_list[20], (SEQS, TOP_K), ((0, 64),), -0.2, 0.2)), 0.1, 1.0)
    expert_gate_weight = centred(key_list[21], (EXPERTS, D, FF), (D // 16) ** -0.5, 0.5, ((0, 64), (2, 4)))
    expert_up_weight = centred(key_list[22], (EXPERTS, D, FF), (D // 16) ** -0.5, 0.5, ((0, 64), (2, 4)))
    expert_down_weight = centred(key_list[23], (EXPERTS, FF, D), (16 * FF) ** -0.5, 0.046875, ((0, 64), (1, 4)))
    return {"tokens": tokens, "previous": previous, "first_norm_gain": first_norm_gain, "token_shift_share": token_shift_share, "receptance_weight": receptance_weight, "key_weight": key_weight, "value_weight": value_weight, "decay_down_map": decay_down_map, "decay_up_map": decay_up_map, "decay_offset": decay_offset, "strength_down_map": strength_down_map, "strength_up_map": strength_up_map, "removal_key_scale": removal_key_scale, "key_damping": key_damping, "self_term_weight": self_term_weight, "head_norm_gain": head_norm_gain, "output_weight": output_weight, "state": state, "second_norm_gain": second_norm_gain, "routes": routes, "chosen_expert_weight": chosen_expert_weight, "expert_gate_weight": expert_gate_weight, "expert_up_weight": expert_up_weight, "expert_down_weight": expert_down_weight}


NORM_EPS = 1e-06
GROUP_EPS = 0.00064
KEY_EPS = 1e-06
GATE_LIMIT = 7.0
GATE_SLOPE = 1.702

def row_rescale(values, gain):
    return values * lax.rsqrt(lax.optimization_barrier(jnp.mean(values * values, axis=-1, keepdims=True)) + NORM_EPS) * gain

def head_combiner(present_rows, prior_rows, first_norm_gain, token_shift_share, receptance_weight, key_weight, value_weight, decay_down_map, decay_up_map, decay_offset, strength_down_map, strength_up_map, removal_key_scale, key_damping, self_term_weight, head_norm_gain, state):
    sequence_count = present_rows.shape[0]
    head_number = state.shape[1]
    head_extent = state.shape[2]
    normed = row_rescale(present_rows.astype(jnp.float32), first_norm_gain)
    before = prior_rows.astype(jnp.float32)

    def shifted(role):
        return (normed + (before - normed) * token_shift_share[role]).astype(jnp.bfloat16)

    def project(inputs, weight):
        return jnp.dot(inputs, weight, preferred_element_type=jnp.float32)

    def by_heads(values):
        return values.reshape(sequence_count, head_number, head_extent)
    receptance_rows = by_heads(project(shifted(0), receptance_weight))
    key_rows = by_heads(project(shifted(1), key_weight))
    value_matrix = by_heads(project(shifted(2), value_weight))
    decay_low = jnp.tanh(project(shifted(3), decay_down_map)).astype(jnp.bfloat16)
    decay_pre = decay_offset + project(decay_low, decay_up_map)
    decay = by_heads(jnp.exp(-jnp.exp(-jax.nn.softplus(-decay_pre) - 0.5)))
    alpha_low = project(shifted(4), strength_down_map).astype(jnp.bfloat16)
    alpha = by_heads(jax.nn.sigmoid(project(alpha_low, strength_up_map)))
    removal = key_rows * removal_key_scale.reshape(head_number, head_extent)
    removal = removal * lax.rsqrt(lax.optimization_barrier(jnp.sum(removal * removal, axis=-1, keepdims=True)) + KEY_EPS)
    blended_rows = key_rows * (1.0 + (alpha - 1.0) * key_damping.reshape(head_number, head_extent))
    highest = lax.Precision.HIGHEST
    along = jnp.einsum('shij,shj->shi', state, removal, precision=highest)
    new_state = state * decay[:, :, None, :] - along[..., None] * (removal * alpha)[:, :, None, :] + value_matrix[..., None] * blended_rows[:, :, None, :]
    readout = jnp.einsum('shij,shj->shi', new_state, receptance_rows, precision=highest)
    centered = readout - lax.optimization_barrier(jnp.mean(readout, axis=-1, keepdims=True))
    variance = lax.optimization_barrier(jnp.mean(centered * centered, axis=-1, keepdims=True))
    heads_normalised = centered * lax.rsqrt(variance + GROUP_EPS) * head_norm_gain.reshape(head_number, head_extent)
    self_term = lax.optimization_barrier(jnp.sum(receptance_rows * blended_rows * self_term_weight, axis=-1, keepdims=True)) * value_matrix
    mixed_inputs = (heads_normalised + self_term).reshape(sequence_count, head_number * head_extent).astype(jnp.bfloat16)
    return (mixed_inputs, new_state)

def split_sum(left, right):
    block_rows = left.shape[1] // N_TP
    total = jnp.zeros((left.shape[0], right.shape[1]), jnp.float32)
    for block_index in range(N_TP):
        lower = block_index * block_rows
        product = jnp.dot(left[:, lower:lower + block_rows], right[lower:lower + block_rows], preferred_element_type=jnp.float32).astype(jnp.bfloat16)
        total = total + lax.optimization_barrier(product).astype(jnp.float32)
    return total

def reference(tokens, previous, first_norm_gain, token_shift_share, receptance_weight, key_weight, value_weight, decay_down_map, decay_up_map, decay_offset, strength_down_map, strength_up_map, removal_key_scale, key_damping, self_term_weight, head_norm_gain, output_weight, state, second_norm_gain, routes, chosen_expert_weight, expert_gate_weight, expert_up_weight, expert_down_weight):
    model_width = tokens.shape[1]

    def one_group(blocks):
        present_rows, prior_rows, state_tile = blocks
        return head_combiner(present_rows, prior_rows, first_norm_gain, token_shift_share, receptance_weight, key_weight, value_weight, decay_down_map, decay_up_map, decay_offset, strength_down_map, strength_up_map, removal_key_scale, key_damping, self_term_weight, head_norm_gain, state_tile)
    mixed_inputs, new_state = lax.map(one_group, (tokens.reshape(N_EP, SEQ_DEV, model_width), previous.reshape(N_EP, SEQ_DEV, model_width), state.reshape(N_EP, SEQ_DEV, HEAD_TOTAL, HEAD_WIDTH, HEAD_WIDTH)))
    mixed_inputs = mixed_inputs.reshape(SEQS, HEAD_TOTAL * HEAD_WIDTH)
    new_state = new_state.reshape(SEQS, HEAD_TOTAL, HEAD_WIDTH, HEAD_WIDTH)
    residual = tokens.astype(jnp.float32) + split_sum(mixed_inputs, output_weight)
    expert_in = row_rescale(residual, second_norm_gain).astype(jnp.bfloat16)
    grouped = routes.reshape(N_EP, SEQ_DEV * TOP_K)
    expert_ids = jnp.arange(EXPERTS, dtype=jnp.int32)
    onehot = (grouped[:, :, None] == expert_ids[None, None, :]).astype(jnp.int32)
    ranking = lax.optimization_barrier(jnp.sum((jnp.cumsum(onehot, axis=1) - onehot) * onehot, axis=2))
    source = jnp.arange(N_EP, dtype=jnp.int32)[:, None]
    slot_index = (grouped * (N_EP * CAP) + source * CAP + ranking).reshape(-1).astype(jnp.int32)
    owner = (jnp.arange(SEQS * TOP_K, dtype=jnp.int32) // TOP_K).astype(jnp.int32)
    buffer = jnp.zeros((EXPERTS * N_EP * CAP, model_width), jnp.bfloat16).at[slot_index].set(expert_in[owner])

    def one_expert(blocks):
        rows_in, gate_weight, up_weight, down_weight = blocks
        gate_pre = jnp.minimum(jnp.dot(rows_in, gate_weight, preferred_element_type=jnp.float32), GATE_LIMIT)
        up_pre = jnp.clip(jnp.dot(rows_in, up_weight, preferred_element_type=jnp.float32), -GATE_LIMIT, GATE_LIMIT)
        activation = ((up_pre + 1.0) * gate_pre * jax.nn.sigmoid(GATE_SLOPE * gate_pre)).astype(jnp.bfloat16)
        return split_sum(activation, down_weight).astype(jnp.bfloat16)
    expert_out = lax.map(one_expert, (buffer.reshape(EXPERTS, N_EP * CAP, model_width), expert_gate_weight, expert_up_weight, expert_down_weight))
    picked = expert_out.reshape(EXPERTS * N_EP * CAP, model_width)[slot_index].astype(jnp.float32)
    picked = picked.reshape(SEQS, TOP_K, model_width)
    layer_out = (residual + lax.optimization_barrier(jnp.sum(picked * chosen_expert_weight[:, :, None], axis=1))).astype(jnp.bfloat16)
    return (layer_out, new_state)
```

```python
import jax
import jax.numpy as jnp
from jax import lax
from jax.experimental import pallas as pl
from jax.experimental.pallas import tpu as pltpu
from jax.sharding import PartitionSpec as P

NORM_EPS = 1e-06
GROUP_EPS = 0.00064
KEY_EPS = 1e-06
GATE_LIMIT = 7.0
GATE_SLOPE = 1.702
CAPACITY = 3


def from_offset(value, offset, axis="tp"):
    devices = lax.axis_size(axis)
    return lax.ppermute(value, axis, [(i, (i - offset) % devices) for i in range(devices)])


def to_offset(value, offset, axis="tp"):
    return from_offset(value, -offset, axis)


def row_rescale(values, gain):
    return values * lax.rsqrt(jnp.mean(values * values, axis=-1, keepdims=True) + NORM_EPS) * gain


def head_combiner(
    present_rows,
    prior_rows,
    first_norm_gain,
    token_shift_share,
    receptance_weight,
    key_weight,
    value_weight,
    decay_down_map,
    decay_up_map,
    decay_offset,
    strength_down_map,
    strength_up_map,
    removal_key_scale,
    key_damping,
    self_term_weight,
    head_norm_gain,
    state,
):
    sequence_count = present_rows.shape[0]
    head_number = state.shape[1]
    head_extent = state.shape[2]
    normed = row_rescale(present_rows.astype(jnp.float32), first_norm_gain)
    before = prior_rows.astype(jnp.float32)

    def shifted(role):
        return (normed + (before - normed) * token_shift_share[role]).astype(jnp.bfloat16)

    def project(inputs, weight):
        return jnp.dot(inputs, weight, preferred_element_type=jnp.float32)

    def by_heads(values):
        return values.reshape(sequence_count, head_number, head_extent)

    receptance_rows = by_heads(project(shifted(0), receptance_weight))
    key_rows = by_heads(project(shifted(1), key_weight))
    value_matrix = by_heads(project(shifted(2), value_weight))
    decay_low = jnp.tanh(project(shifted(3), decay_down_map)).astype(jnp.bfloat16)
    decay_pre = decay_offset + project(decay_low, decay_up_map)
    decay = by_heads(jnp.exp(-jnp.exp(-jax.nn.softplus(-decay_pre) - 0.5)))
    alpha_low = project(shifted(4), strength_down_map).astype(jnp.bfloat16)
    alpha = by_heads(jax.nn.sigmoid(project(alpha_low, strength_up_map)))
    removal = key_rows * removal_key_scale.reshape(head_number, head_extent)
    removal = removal * lax.rsqrt(jnp.sum(removal * removal, axis=-1, keepdims=True) + KEY_EPS)
    blended_rows = key_rows * (1.0 + (alpha - 1.0) * key_damping.reshape(head_number, head_extent))
    along = jnp.einsum("shij,shj->shi", state, removal)
    kept = jnp.einsum("shij,shj->shi", state, decay * receptance_rows)
    readout = (
        kept
        - along * jnp.sum(removal * alpha * receptance_rows, axis=-1, keepdims=True)
        + value_matrix * jnp.sum(blended_rows * receptance_rows, axis=-1, keepdims=True)
    )
    new_state = (
        state * decay[:, :, None, :]
        - along[..., None] * (removal * alpha)[:, :, None, :]
        + value_matrix[..., None] * blended_rows[:, :, None, :]
    )
    centered = readout - jnp.mean(readout, axis=-1, keepdims=True)
    variance = jnp.mean(centered * centered, axis=-1, keepdims=True)
    heads_normalised = (
        centered
        * lax.rsqrt(variance + GROUP_EPS)
        * head_norm_gain.reshape(head_number, head_extent)
    )
    self_term = (
        jnp.sum(receptance_rows * blended_rows * self_term_weight, axis=-1, keepdims=True)
        * value_matrix
    )
    mixed_inputs = (
        (heads_normalised + self_term)
        .reshape(sequence_count, head_number * head_extent)
        .astype(jnp.bfloat16)
    )
    return (mixed_inputs, new_state)


def hidden_kernel(at, x0, x1, x2, x3, gain, gate_weight, up_weight, out):
    pieces = (x0, x1, x2, x3)
    width = x0.shape[1]
    places = [lax.rem(at[0] + k, 4) * width for k in range(4)]
    floats = [x[...].astype(jnp.float32) for x in pieces]
    squares = sum(jnp.sum(f * f, axis=1, keepdims=True) for f in floats)
    scale = lax.rsqrt(squares / (4 * width) + NORM_EPS)
    gate = jnp.zeros(out.shape, jnp.float32)
    up = jnp.zeros(out.shape, jnp.float32)
    for f, place in zip(floats, places):
        rows = pl.ds(pl.multiple_of(place, width), width)
        x = (f * scale * gain[:, rows]).astype(jnp.bfloat16)
        gate = gate + jnp.dot(x, gate_weight[rows, :], preferred_element_type=jnp.float32)
        up = up + jnp.dot(x, up_weight[rows, :], preferred_element_type=jnp.float32)
    gate = jnp.minimum(gate, GATE_LIMIT)
    up = jnp.clip(up, -GATE_LIMIT, GATE_LIMIT)
    out[...] = ((up + 1.0) * gate * jax.nn.sigmoid(GATE_SLOPE * gate)).astype(jnp.bfloat16)


def down_kernel(a0, a1, a2, a3, w0, w1, w2, w3, out):
    total = jnp.zeros(out.shape, jnp.float32)
    for a, w in ((a0, w0), (a1, w1), (a2, w2), (a3, w3)):
        total = total + jnp.dot(a[...], w[...], preferred_element_type=jnp.float32)
    out[...] = total.astype(jnp.bfloat16)


def in_vmem(count):
    return [pl.BlockSpec(memory_space=pltpu.VMEM)] * count


def shards(
    tokens,
    previous,
    first_norm_gain,
    token_shift_share,
    receptance_weight,
    key_weight,
    value_weight,
    decay_down_map,
    decay_up_map,
    decay_offset,
    strength_down_map,
    strength_up_map,
    removal_key_scale,
    key_damping,
    self_term_weight,
    head_norm_gain,
    output_weight,
    state,
    second_norm_gain,
    routes,
    chosen_expert_weight,
    expert_gate_weight,
    expert_up_weight,
    expert_down_weight,
):
    at = lax.axis_index("tp")
    sequences, own_columns = tokens.shape
    both = jnp.concatenate([tokens, previous], axis=0)
    pieces = [both] + [from_offset(both, k) for k in (1, 2, 3)]
    rotated = jnp.concatenate(pieces + pieces[:3], axis=1)
    everyone = lax.dynamic_slice_in_dim(
        rotated, lax.rem(4 - at, 4) * own_columns, 4 * own_columns, 1
    )
    present_rows, prior_rows = everyone[:sequences], everyone[sequences:]

    experts = expert_gate_weight.shape[0] * lax.axis_size("ep")
    ids = jnp.arange(experts, dtype=jnp.int32)
    hits = routes[:, :, None] == ids[None, None, :]
    named = jnp.sum(hits.astype(jnp.float32), axis=1)
    earlier = jnp.tril(jnp.ones((sequences, sequences), jnp.float32), -1)
    ranking = jnp.dot(earlier, named)
    weight_of = jnp.sum(jnp.where(hits, chosen_expert_weight[:, :, None], 0.0), axis=1)
    slots = [(ranking == c) & (named > 0) for c in range(CAPACITY)]
    dispatch = jnp.concatenate([s.astype(jnp.bfloat16) for s in slots], axis=1)
    combine = jnp.concatenate([jnp.where(s, weight_of, 0.0) for s in slots], axis=1)

    head_columns = receptance_weight.shape[1]
    decay_own = lax.dynamic_slice_in_dim(decay_up_map, at * head_columns, head_columns, 1)
    alpha_own = lax.dynamic_slice_in_dim(strength_up_map, at * head_columns, head_columns, 1)
    mixed_inputs, new_state = head_combiner(
        present_rows,
        prior_rows,
        first_norm_gain,
        token_shift_share,
        receptance_weight,
        key_weight,
        value_weight,
        decay_down_map,
        decay_own,
        decay_offset,
        strength_down_map,
        alpha_own,
        removal_key_scale,
        key_damping,
        self_term_weight,
        head_norm_gain,
        state,
    )
    head_terms = jnp.dot(
        mixed_inputs, output_weight, preferred_element_type=jnp.float32
    ).astype(jnp.bfloat16)
    down_weight = expert_down_weight[0]

    def columns_of(value, k):
        return lax.dynamic_slice_in_dim(value, lax.rem(at + k, 4) * own_columns, own_columns, 1)

    arrived = [columns_of(head_terms, 0)] + [
        to_offset(columns_of(head_terms, k), k) for k in (1, 2, 3)
    ]
    residual = tokens.astype(jnp.float32) + sum(a.astype(jnp.float32) for a in arrived)
    down_tied, head_tied = lax.optimization_barrier((down_weight, head_terms))
    down_pieces = [columns_of(down_weight, 0)] + [
        to_offset(columns_of(down_tied, k), k) for k in (1, 2, 3)
    ]

    outgoing = lax.dot_general(
        dispatch,
        residual.astype(jnp.bfloat16),
        (((0,), (0,)), ((), ())),
        preferred_element_type=jnp.float32,
    ).astype(jnp.bfloat16)
    outgoing = outgoing.reshape(CAPACITY, experts, own_columns)
    came = lax.all_to_all(outgoing, "ep", split_axis=1, concat_axis=1, tiled=True)
    own_rows = came.reshape(CAPACITY * experts, own_columns)
    row_pieces = [own_rows] + [from_offset(own_rows, k) for k in (1, 2, 3)]
    hidden_columns = expert_gate_weight.shape[2]
    activation = pl.pallas_call(
        hidden_kernel,
        out_shape=jax.ShapeDtypeStruct((own_rows.shape[0], hidden_columns), jnp.bfloat16),
        in_specs=[pl.BlockSpec(memory_space=pltpu.SMEM)] + in_vmem(7),
        out_specs=pl.BlockSpec(memory_space=pltpu.VMEM),
        name="hidden",
    )(
        at[None],
        *row_pieces,
        second_norm_gain[None, :],
        expert_gate_weight[0],
        expert_up_weight[0],
    )
    act_pieces = [activation] + [to_offset(activation, k) for k in (1, 2, 3)]
    shares = pl.pallas_call(
        down_kernel,
        out_shape=jax.ShapeDtypeStruct((own_rows.shape[0], own_columns), jnp.bfloat16),
        in_specs=in_vmem(8),
        out_specs=pl.BlockSpec(memory_space=pltpu.VMEM),
        name="down",
    )(*act_pieces, *down_pieces)
    shares = shares.reshape(CAPACITY, experts, own_columns)
    returned = lax.all_to_all(shares, "ep", split_axis=1, concat_axis=1, tiled=True)
    returned = returned.reshape(CAPACITY * experts, own_columns)
    high = combine.astype(jnp.bfloat16)
    low = (combine - high.astype(jnp.float32)).astype(jnp.bfloat16)
    weighted = jnp.dot(
        jnp.concatenate([high, low], axis=0), returned, preferred_element_type=jnp.float32
    )
    layer_out = (residual + weighted[:sequences] + weighted[sequences:]).astype(jnp.bfloat16)
    return (layer_out, new_state)


def solution(mesh):
    in_specs = (
        P("ep", "tp"),
        P("ep", "tp"),
        P(),
        P(),
        P(None, "tp"),
        P(None, "tp"),
        P(None, "tp"),
        P(),
        P(),
        P("tp"),
        P(),
        P(),
        P("tp"),
        P("tp"),
        P("tp", None),
        P("tp"),
        P("tp", None),
        P("ep", "tp", None, None),
        P(),
        P("ep", None),
        P("ep", None),
        P("ep", None, "tp"),
        P("ep", None, "tp"),
        P("ep", "tp", None),
    )
    out_specs = (P("ep", "tp"), P("ep", "tp", None, None))
    return jax.shard_map(shards, mesh=mesh, in_specs=in_specs, out_specs=out_specs, check_vma=False)
```

```python
import math

import jax
import jax.numpy as jnp
from jax import lax
from jax.experimental import pallas as pl
from jax.experimental.pallas import tpu as pltpu
from jax.sharding import PartitionSpec as P

NORM_EPS = 1e-06
GROUP_EPS = 0.00064
KEY_EPS = 1e-06
GATE_LIMIT = 7.0
GATE_SLOPE = 1.702
CAPACITY = 3
HALF_DECAY = math.exp(-0.5)
MIB = 1 << 20


def from_offset(value, offset, axis="tp"):
    devices = lax.axis_size(axis)
    return lax.ppermute(value, axis, [(i, (i - offset) % devices) for i in range(devices)])


def to_offset(value, offset, axis="tp"):
    return from_offset(value, -offset, axis)


def head_sums(values, same_head):
    high = values.astype(jnp.bfloat16)
    low = (values - high.astype(jnp.float32)).astype(jnp.bfloat16)
    return jnp.dot(high, same_head, preferred_element_type=jnp.float32) + jnp.dot(
        low, same_head, preferred_element_type=jnp.float32
    )


def attention_kernel(
    at,
    p0,
    p1,
    p2,
    p3,
    first_gain,
    share,
    receptance_weight,
    key_weight,
    value_weight,
    decay_down,
    decay_up,
    decay_offset,
    strength_down,
    strength_up,
    removal_scale,
    damping,
    self_weight,
    head_gain,
    output_weight,
    state,
    o0,
    o1,
    o2,
    o3,
    decay_out,
    removal_out,
    along_out,
    value_out,
    blended_out,
    vectors,
    results,
):
    sequences, columns = decay_out.shape
    heads, width = self_weight.shape
    block = p0.shape[1]
    places = [pl.multiple_of(lax.rem(at[0] + k, 4) * block, block) for k in range(4)]
    present = [p[:sequences, :].astype(jnp.float32) for p in (p0, p1, p2, p3)]
    prior = [p[sequences:, :].astype(jnp.float32) for p in (p0, p1, p2, p3)]
    squares = sum(jnp.sum(x * x, axis=1, keepdims=True) for x in present)
    scale = lax.rsqrt(squares / (4 * block) + NORM_EPS)
    weights = (receptance_weight, key_weight, value_weight, decay_down, strength_down)
    sums = [None] * 5
    for place, x, b in zip(places, present, prior):
        rows = pl.ds(place, block)
        normed = x * scale * first_gain[:, rows]
        change = b - normed
        for m, weight in enumerate(weights):
            moved = (normed + change * share[m : m + 1, rows]).astype(jnp.bfloat16)
            part = jnp.dot(moved, weight[rows, :], preferred_element_type=jnp.float32)
            sums[m] = part if sums[m] is None else sums[m] + part
    receptance, key, value, decay_low, strength_low = sums
    own = pl.ds(pl.multiple_of(at[0] * columns, columns), columns)
    decay_pre = decay_offset[...] + jnp.dot(
        jnp.tanh(decay_low).astype(jnp.bfloat16),
        decay_up[:, own],
        preferred_element_type=jnp.float32,
    )
    decay = jnp.exp(-HALF_DECAY * jax.nn.sigmoid(decay_pre))
    alpha = jax.nn.sigmoid(
        jnp.dot(
            strength_low.astype(jnp.bfloat16),
            strength_up[:, own],
            preferred_element_type=jnp.float32,
        )
    )
    lane = lax.broadcasted_iota(jnp.int32, (columns, columns), 1) // width
    row = lax.broadcasted_iota(jnp.int32, (columns, columns), 0) // width
    same_head = (lane == row).astype(jnp.bfloat16)
    removal = key * removal_scale[...]
    removal = removal * lax.rsqrt(head_sums(removal * removal, same_head) + KEY_EPS)
    blended = key * (1.0 + (alpha - 1.0) * damping[...])
    removed = removal * alpha
    pair = 2 * width
    rows_each = 2 * heads
    for v, vector in enumerate((removal, decay * receptance)):
        for h in range(heads):
            two = vector[:, h // 2 * pair : h // 2 * pair + pair]
            vectors[pl.ds(v * heads + h, sequences, stride=rows_each), :] = (
                pltpu.roll(two, width, 1) if h % 2 else two
            )
    for s in range(sequences):
        rows = pl.ds(s * rows_each, rows_each)
        found = lax.dot_general(
            vectors[rows, :][:, :width].astype(jnp.bfloat16),
            state[s].astype(jnp.bfloat16),
            (((1,), (1,)), ((), ())),
            preferred_element_type=jnp.float32,
        )
        for c in range(heads // 2):
            results[c, rows, :] = found[:, c * pair : (c + 1) * pair]
    first_of_two = lax.broadcasted_iota(jnp.int32, (sequences, pair), 1) < width

    def of_vector(v):
        parts = []
        for c in range(heads // 2):
            one, other = (
                results[c, pl.ds(v * heads + 2 * c + i, sequences, stride=rows_each), :]
                for i in (0, 1)
            )
            parts.append(jnp.where(first_of_two, one, other))
        return jnp.concatenate(parts, axis=1)

    along, kept = of_vector(0), of_vector(1)
    gains = jnp.concatenate([self_weight[h : h + 1, :] for h in range(heads)], axis=1)
    readout = (
        kept
        - along * head_sums(removed * receptance, same_head)
        + value * head_sums(blended * receptance, same_head)
    )
    centered = readout - head_sums(readout, same_head) / width
    variance = head_sums(centered * centered, same_head) / width
    mixed = (
        centered * lax.rsqrt(variance + GROUP_EPS) * head_gain[...]
        + head_sums(receptance * blended * gains, same_head) * value
    ).astype(jnp.bfloat16)
    for place, o in zip(places, (o0, o1, o2, o3)):
        o[...] = jnp.dot(
            mixed, output_weight[:, pl.ds(place, block)], preferred_element_type=jnp.float32
        ).astype(jnp.bfloat16)
    decay_out[...] = decay
    removal_out[...] = removed
    along_out[...] = along
    value_out[...] = value
    blended_out[...] = blended


def stack_kernel(first, second, out, sems):
    height = first.shape[0]
    copies = [
        pltpu.make_async_copy(first, out.at[pl.ds(0, height)], sems.at[0]),
        pltpu.make_async_copy(second, out.at[pl.ds(height, height)], sems.at[1]),
    ]
    for copy in copies:
        copy.start()
    for copy in copies:
        copy.wait()


def fetch_kernel(*refs):
    count = len(refs) // 2
    sems = refs[-1]
    copies = [
        pltpu.make_async_copy(refs[i], refs[count + i], sems.at[i]) for i in range(count)
    ]
    for copy in copies:
        copy.start()
    for copy in copies:
        copy.wait()


def from_hbm(kernel, name, shapes, count, limit):
    call = pl.pallas_call(
        kernel,
        out_shape=shapes,
        in_specs=[pl.BlockSpec(memory_space=pltpu.HBM)] * count,
        out_specs=jax.tree.map(lambda _: pl.BlockSpec(memory_space=pltpu.VMEM), shapes),
        scratch_shapes=[pltpu.SemaphoreType.DMA((count,))],
        compiler_params=pltpu.CompilerParams(vmem_limit_bytes=limit * MIB),
        name=name,
    )
    return lambda *values: call(
        *[pltpu.with_memory_space_constraint(value, pltpu.HBM) for value in values]
    )


def hidden_kernel(at, x0, x1, x2, x3, gain, gate_weight, up_weight, out):
    pieces = (x0, x1, x2, x3)
    width = x0.shape[1]
    places = [lax.rem(at[0] + k, 4) * width for k in range(4)]
    floats = [x[...].astype(jnp.float32) for x in pieces]
    squares = sum(jnp.sum(f * f, axis=1, keepdims=True) for f in floats)
    scale = lax.rsqrt(squares / (4 * width) + NORM_EPS)
    gate = jnp.zeros(out.shape, jnp.float32)
    up = jnp.zeros(out.shape, jnp.float32)
    for f, place in zip(floats, places):
        rows = pl.ds(pl.multiple_of(place, width), width)
        x = (f * scale * gain[:, rows]).astype(jnp.bfloat16)
        gate = gate + jnp.dot(x, gate_weight[rows, :], preferred_element_type=jnp.float32)
        up = up + jnp.dot(x, up_weight[rows, :], preferred_element_type=jnp.float32)
    gate = jnp.minimum(gate, GATE_LIMIT)
    up = jnp.clip(up, -GATE_LIMIT, GATE_LIMIT)
    out[...] = ((up + 1.0) * gate * jax.nn.sigmoid(GATE_SLOPE * gate)).astype(jnp.bfloat16)


def down_kernel(at, activation, down_weight, o0, o1, o2, o3):
    block = o0.shape[1]
    for k, o in enumerate((o0, o1, o2, o3)):
        place = pl.multiple_of(lax.rem(at[0] + k, 4) * block, block)
        o[...] = jnp.dot(
            activation[...],
            down_weight[:, pl.ds(place, block)],
            preferred_element_type=jnp.float32,
        ).astype(jnp.bfloat16)


def local_call(kernel, name, shapes, limit, scratch=()):
    def call(at, *operands):
        in_vmem = pl.BlockSpec(memory_space=pltpu.VMEM)
        return pl.pallas_call(
            kernel,
            out_shape=shapes,
            in_specs=[pl.BlockSpec(memory_space=pltpu.SMEM)] + [in_vmem] * len(operands),
            out_specs=jax.tree.map(lambda _: in_vmem, shapes),
            scratch_shapes=scratch,
            compiler_params=pltpu.CompilerParams(vmem_limit_bytes=limit * MIB),
            name=name,
        )(at, *operands)

    return call


def shards(
    tokens,
    previous,
    first_norm_gain,
    token_shift_share,
    receptance_weight,
    key_weight,
    value_weight,
    decay_down_map,
    decay_up_map,
    decay_offset,
    strength_down_map,
    strength_up_map,
    removal_key_scale,
    key_damping,
    self_term_weight,
    head_norm_gain,
    output_weight,
    state,
    second_norm_gain,
    routes,
    chosen_expert_weight,
    expert_gate_weight,
    expert_up_weight,
    expert_down_weight,
):
    at = lax.axis_index("tp")[None]
    sequences, own_columns = tokens.shape
    head_columns = receptance_weight.shape[1]
    float32 = lambda *shape: jax.ShapeDtypeStruct(shape, jnp.float32)
    bfloat16 = lambda *shape: jax.ShapeDtypeStruct(shape, jnp.bfloat16)
    both = from_hbm(
        stack_kernel, "stack", jax.ShapeDtypeStruct((2 * sequences, own_columns), tokens.dtype), 2, 1
    )(tokens, previous)
    row_pieces = [both] + [from_offset(both, k) for k in (1, 2, 3)]

    vector = lambda value: value[None, :]
    needed = (
        vector(first_norm_gain),
        token_shift_share,
        receptance_weight,
        key_weight,
        value_weight,
        decay_down_map,
        decay_up_map,
        vector(decay_offset),
        strength_down_map,
        strength_up_map,
        vector(removal_key_scale),
        vector(key_damping),
        self_term_weight,
        vector(head_norm_gain),
        output_weight,
        state.reshape(sequences, head_columns, state.shape[3]),
    )
    needed = from_hbm(
        fetch_kernel,
        "fetch",
        [jax.ShapeDtypeStruct(a.shape, a.dtype) for a in needed],
        len(needed),
        16,
    )(*needed)

    experts = expert_gate_weight.shape[0] * lax.axis_size("ep")
    ids = jnp.arange(experts, dtype=jnp.int32)
    hits = routes[:, :, None] == ids[None, None, :]
    named = jnp.sum(hits.astype(jnp.float32), axis=1)
    earlier = jnp.tril(jnp.ones((sequences, sequences), jnp.float32), -1)
    ranking = jnp.dot(earlier, named)
    weight_of = jnp.sum(jnp.where(hits, chosen_expert_weight[:, :, None], 0.0), axis=1)
    slots = [(ranking == c) & (named > 0) for c in range(CAPACITY)]
    dispatch = jnp.concatenate([s.astype(jnp.bfloat16) for s in slots], axis=1)
    combine = jnp.concatenate([jnp.where(s, weight_of, 0.0) for s in slots], axis=1)

    *head_terms, decay, removed, along, value, blended = local_call(
        attention_kernel,
        "attention",
        [bfloat16(sequences, own_columns)] * 4 + [float32(sequences, head_columns)] * 5,
        24,
        [
            pltpu.VMEM((8 * sequences, 128), jnp.float32),
            pltpu.VMEM((2, 8 * sequences, 128), jnp.float32),
        ],
    )(
        at,
        *row_pieces,
        *needed,
    )
    by_heads = lambda value: value.reshape(state.shape[:3])
    new_state = (
        state * by_heads(decay)[:, :, None, :]
        - by_heads(along)[..., None] * by_heads(removed)[:, :, None, :]
        + by_heads(value)[..., None] * by_heads(blended)[:, :, None, :]
    )
    arrived = [head_terms[0]] + [to_offset(head_terms[k], k) for k in (1, 2, 3)]
    residual = tokens.astype(jnp.float32) + sum(a.astype(jnp.float32) for a in arrived)

    outgoing = lax.dot_general(
        dispatch,
        residual.astype(jnp.bfloat16),
        (((0,), (0,)), ((), ())),
        preferred_element_type=jnp.float32,
    ).astype(jnp.bfloat16)
    outgoing = outgoing.reshape(CAPACITY, experts, own_columns)
    came = lax.all_to_all(outgoing, "ep", split_axis=1, concat_axis=1, tiled=True)
    own_rows = came.reshape(CAPACITY * experts, own_columns)
    row_pieces = [own_rows] + [from_offset(own_rows, k) for k in (1, 2, 3)]
    activation = local_call(
        hidden_kernel, "hidden", bfloat16(own_rows.shape[0], expert_gate_weight.shape[2]), 12
    )(
        at,
        *row_pieces,
        vector(second_norm_gain),
        expert_gate_weight[0],
        expert_up_weight[0],
    )
    down_terms = local_call(
        down_kernel, "down", [bfloat16(own_rows.shape[0], own_columns)] * 4, 8
    )(at, activation, expert_down_weight[0])
    arrived = [down_terms[0]] + [to_offset(down_terms[k], k) for k in (1, 2, 3)]
    shares = sum(a.astype(jnp.float32) for a in arrived).astype(jnp.bfloat16)
    shares = shares.reshape(CAPACITY, experts, own_columns)
    returned = lax.all_to_all(shares, "ep", split_axis=1, concat_axis=1, tiled=True)
    returned = returned.reshape(CAPACITY * experts, own_columns)
    high = combine.astype(jnp.bfloat16)
    low = (combine - high.astype(jnp.float32)).astype(jnp.bfloat16)
    weighted = jnp.dot(
        jnp.concatenate([high, low], axis=0), returned, preferred_element_type=jnp.float32
    )
    layer_out = (residual + weighted[:sequences] + weighted[sequences:]).astype(jnp.bfloat16)
    return (layer_out, new_state)


def solution(mesh):
    in_specs = (
        P("ep", "tp"),
        P("ep", "tp"),
        P(),
        P(),
        P(None, "tp"),
        P(None, "tp"),
        P(None, "tp"),
        P(),
        P(),
        P("tp"),
        P(),
        P(),
        P("tp"),
        P("tp"),
        P("tp", None),
        P("tp"),
        P("tp", None),
        P("ep", "tp", None, None),
        P(),
        P("ep", None),
        P("ep", None),
        P("ep", None, "tp"),
        P("ep", None, "tp"),
        P("ep", "tp", None),
    )
    out_specs = (P("ep", "tp"), P("ep", "tp", None, None))
    return jax.shard_map(shards, mesh=mesh, in_specs=in_specs, out_specs=out_specs, check_vma=False)
```

```python
import math

import jax
import jax.numpy as jnp
from jax import lax
from jax.experimental import pallas as pl
from jax.experimental.pallas import tpu as pltpu
from jax.sharding import PartitionSpec as P

NORM_EPS = 1e-06
GROUP_EPS = 0.00064
KEY_EPS = 1e-06
GATE_LIMIT = 7.0
GATE_SLOPE = 1.702
CAPACITY = 3
HALF_DECAY = math.exp(-0.5)
MIB = 1 << 20


def from_offset(value, offset, axis="tp"):
    devices = lax.axis_size(axis)
    return lax.ppermute(value, axis, [(i, (i - offset) % devices) for i in range(devices)])


def to_offset(value, offset, axis="tp"):
    return from_offset(value, -offset, axis)


def gathered(value):
    pieces = {k: from_offset(value, k) for k in (1, 3, 2)}
    return [value, pieces[1], pieces[2], pieces[3]]


def scattered(values):
    pieces = {k: to_offset(values[k], k) for k in (1, 3, 2)}
    return [values[0], pieces[1], pieces[2], pieces[3]]


def head_sums(values, same_head):
    high = values.astype(jnp.bfloat16)
    low = (values - high.astype(jnp.float32)).astype(jnp.bfloat16)
    return jnp.dot(high, same_head, preferred_element_type=jnp.float32) + jnp.dot(
        low, same_head, preferred_element_type=jnp.float32
    )


def attention_kernel(
    at,
    p0,
    p1,
    p2,
    p3,
    first_gain,
    share,
    receptance_weight,
    key_weight,
    value_weight,
    decay_down,
    decay_up,
    decay_offset,
    strength_down,
    strength_up,
    removal_scale,
    damping,
    self_weight,
    head_gain,
    output_weight_hbm,
    state_hbm,
    o0,
    o1,
    o2,
    o3,
    decay_out,
    removal_out,
    along_out,
    value_out,
    blended_out,
    vectors,
    results,
    output_weight,
    state,
    sems,
):
    state_copy = pltpu.make_async_copy(state_hbm, state, sems.at[0])
    state_copy.start()
    weight_copy = pltpu.make_async_copy(output_weight_hbm, output_weight, sems.at[1])
    weight_copy.start()
    sequences, columns = decay_out.shape
    heads, width = self_weight.shape
    block = p0.shape[1]
    places = [pl.multiple_of(lax.rem(at[0] + k, 4) * block, block) for k in range(4)]
    present = [p[:sequences, :].astype(jnp.float32) for p in (p0, p1, p2, p3)]
    prior = [p[sequences:, :].astype(jnp.float32) for p in (p0, p1, p2, p3)]
    squares = sum(jnp.sum(x * x, axis=1, keepdims=True) for x in present)
    scale = lax.rsqrt(squares / (4 * block) + NORM_EPS)
    weights = (receptance_weight, key_weight, value_weight, decay_down, strength_down)
    sums = [None] * 5
    for place, x, b in zip(places, present, prior):
        rows = pl.ds(place, block)
        normed = x * scale * first_gain[:, rows]
        change = b - normed
        for m, weight in enumerate(weights):
            moved = (normed + change * share[m : m + 1, rows]).astype(jnp.bfloat16)
            part = jnp.dot(moved, weight[rows, :], preferred_element_type=jnp.float32)
            sums[m] = part if sums[m] is None else sums[m] + part
    receptance, key, value, decay_low, strength_low = sums
    own = pl.ds(pl.multiple_of(at[0] * columns, columns), columns)
    decay_pre = decay_offset[...] + jnp.dot(
        jnp.tanh(decay_low).astype(jnp.bfloat16),
        decay_up[:, own],
        preferred_element_type=jnp.float32,
    )
    decay = jnp.exp(-HALF_DECAY * jax.nn.sigmoid(decay_pre))
    alpha = jax.nn.sigmoid(
        jnp.dot(
            strength_low.astype(jnp.bfloat16),
            strength_up[:, own],
            preferred_element_type=jnp.float32,
        )
    )
    lane = lax.broadcasted_iota(jnp.int32, (columns, columns), 1) // width
    row = lax.broadcasted_iota(jnp.int32, (columns, columns), 0) // width
    same_head = (lane == row).astype(jnp.bfloat16)
    removal = key * removal_scale[...]
    removal = removal * lax.rsqrt(head_sums(removal * removal, same_head) + KEY_EPS)
    blended = key * (1.0 + (alpha - 1.0) * damping[...])
    removed = removal * alpha
    pair = 2 * width
    rows_each = 2 * heads
    for v, vector in enumerate((removal, decay * receptance)):
        for h in range(heads):
            two = vector[:, h // 2 * pair : h // 2 * pair + pair]
            vectors[pl.ds(v * heads + h, sequences, stride=rows_each), :] = (
                pltpu.roll(two, width, 1) if h % 2 else two
            )
    state_copy.wait()
    for s in range(sequences):
        rows = pl.ds(s * rows_each, rows_each)
        found = lax.dot_general(
            vectors[rows, :][:, :width].astype(jnp.bfloat16),
            state[s].astype(jnp.bfloat16),
            (((1,), (1,)), ((), ())),
            preferred_element_type=jnp.float32,
        )
        for c in range(heads // 2):
            results[c, rows, :] = found[:, c * pair : (c + 1) * pair]
    first_of_two = lax.broadcasted_iota(jnp.int32, (sequences, pair), 1) < width

    def of_vector(v):
        parts = []
        for c in range(heads // 2):
            one, other = (
                results[c, pl.ds(v * heads + 2 * c + i, sequences, stride=rows_each), :]
                for i in (0, 1)
            )
            parts.append(jnp.where(first_of_two, one, other))
        return jnp.concatenate(parts, axis=1)

    along, kept = of_vector(0), of_vector(1)
    gains = jnp.concatenate([self_weight[h : h + 1, :] for h in range(heads)], axis=1)
    readout = (
        kept
        - along * head_sums(removed * receptance, same_head)
        + value * head_sums(blended * receptance, same_head)
    )
    centered = readout - head_sums(readout, same_head) / width
    variance = head_sums(centered * centered, same_head) / width
    mixed = (
        centered * lax.rsqrt(variance + GROUP_EPS) * head_gain[...]
        + head_sums(receptance * blended * gains, same_head) * value
    ).astype(jnp.bfloat16)
    weight_copy.wait()
    for place, o in zip(places, (o0, o1, o2, o3)):
        o[...] = jnp.dot(
            mixed, output_weight[:, pl.ds(place, block)], preferred_element_type=jnp.float32
        ).astype(jnp.bfloat16)
    decay_out[...] = decay
    removal_out[...] = removed
    along_out[...] = along
    value_out[...] = value
    blended_out[...] = blended


def stack_kernel(first, second, out, sems):
    height = first.shape[0]
    copies = [
        pltpu.make_async_copy(first, out.at[pl.ds(0, height)], sems.at[0]),
        pltpu.make_async_copy(second, out.at[pl.ds(height, height)], sems.at[1]),
    ]
    for copy in copies:
        copy.start()
    for copy in copies:
        copy.wait()


def fetch_kernel(*refs):
    count = len(refs) // 2
    sems = refs[-1]
    copies = [
        pltpu.make_async_copy(refs[i], refs[count + i], sems.at[i]) for i in range(count)
    ]
    for copy in copies:
        copy.start()
    for copy in copies:
        copy.wait()


def from_hbm(kernel, name, shapes, count, limit):
    call = pl.pallas_call(
        kernel,
        out_shape=shapes,
        in_specs=[pl.BlockSpec(memory_space=pltpu.HBM)] * count,
        out_specs=jax.tree.map(lambda _: pl.BlockSpec(memory_space=pltpu.VMEM), shapes),
        scratch_shapes=[pltpu.SemaphoreType.DMA((count,))],
        compiler_params=pltpu.CompilerParams(vmem_limit_bytes=limit * MIB),
        name=name,
    )
    return lambda *values: call(
        *[pltpu.with_memory_space_constraint(value, pltpu.HBM) for value in values]
    )


def hidden_kernel(at, x0, x1, x2, x3, gain, gate_weight, up_weight, out):
    pieces = (x0, x1, x2, x3)
    width = x0.shape[1]
    places = [lax.rem(at[0] + k, 4) * width for k in range(4)]
    floats = [x[...].astype(jnp.float32) for x in pieces]
    squares = sum(jnp.sum(f * f, axis=1, keepdims=True) for f in floats)
    scale = lax.rsqrt(squares / (4 * width) + NORM_EPS)
    gate = jnp.zeros(out.shape, jnp.float32)
    up = jnp.zeros(out.shape, jnp.float32)
    for f, place in zip(floats, places):
        rows = pl.ds(pl.multiple_of(place, width), width)
        x = (f * scale * gain[:, rows]).astype(jnp.bfloat16)
        gate = gate + jnp.dot(x, gate_weight[rows, :], preferred_element_type=jnp.float32)
        up = up + jnp.dot(x, up_weight[rows, :], preferred_element_type=jnp.float32)
    gate = jnp.minimum(gate, GATE_LIMIT)
    up = jnp.clip(up, -GATE_LIMIT, GATE_LIMIT)
    out[...] = ((up + 1.0) * gate * jax.nn.sigmoid(GATE_SLOPE * gate)).astype(jnp.bfloat16)


def down_kernel(at, activation, down_weight, o0, o1, o2, o3):
    block = o0.shape[1]
    for k, o in enumerate((o0, o1, o2, o3)):
        place = pl.multiple_of(lax.rem(at[0] + k, 4) * block, block)
        o[...] = jnp.dot(
            activation[...],
            down_weight[:, pl.ds(place, block)],
            preferred_element_type=jnp.float32,
        ).astype(jnp.bfloat16)


def local_call(kernel, name, shapes, limit, scratch=(), left=0):
    def call(at, *operands):
        in_vmem = pl.BlockSpec(memory_space=pltpu.VMEM)
        count = len(operands) - left
        operands = operands[:count] + tuple(
            pltpu.with_memory_space_constraint(value, pltpu.HBM) for value in operands[count:]
        )
        return pl.pallas_call(
            kernel,
            out_shape=shapes,
            in_specs=[pl.BlockSpec(memory_space=pltpu.SMEM)]
            + [in_vmem] * count
            + [pl.BlockSpec(memory_space=pltpu.HBM)] * left,
            out_specs=jax.tree.map(lambda _: in_vmem, shapes),
            scratch_shapes=scratch,
            compiler_params=pltpu.CompilerParams(vmem_limit_bytes=limit * MIB),
            name=name,
        )(at, *operands)

    return call


def shards(
    tokens,
    previous,
    first_norm_gain,
    token_shift_share,
    receptance_weight,
    key_weight,
    value_weight,
    decay_down_map,
    decay_up_map,
    decay_offset,
    strength_down_map,
    strength_up_map,
    removal_key_scale,
    key_damping,
    self_term_weight,
    head_norm_gain,
    output_weight,
    state,
    second_norm_gain,
    routes,
    chosen_expert_weight,
    expert_gate_weight,
    expert_up_weight,
    expert_down_weight,
):
    at = lax.axis_index("tp")[None]
    sequences, own_columns = tokens.shape
    head_columns = receptance_weight.shape[1]
    float32 = lambda *shape: jax.ShapeDtypeStruct(shape, jnp.float32)
    bfloat16 = lambda *shape: jax.ShapeDtypeStruct(shape, jnp.bfloat16)
    both = from_hbm(
        stack_kernel, "stack", jax.ShapeDtypeStruct((2 * sequences, own_columns), tokens.dtype), 2, 1
    )(tokens, previous)
    row_pieces = gathered(both)

    vector = lambda value: value[None, :]
    needed = (
        vector(first_norm_gain),
        token_shift_share,
        receptance_weight,
        key_weight,
        value_weight,
        decay_down_map,
        decay_up_map,
        vector(decay_offset),
        strength_down_map,
        strength_up_map,
        vector(removal_key_scale),
        vector(key_damping),
        self_term_weight,
        vector(head_norm_gain),
    )
    needed = from_hbm(
        fetch_kernel,
        "fetch",
        [jax.ShapeDtypeStruct(a.shape, a.dtype) for a in needed],
        len(needed),
        12,
    )(*needed)

    experts = expert_gate_weight.shape[0] * lax.axis_size("ep")
    ids = jnp.arange(experts, dtype=jnp.int32)
    hits = routes[:, :, None] == ids[None, None, :]
    named = jnp.sum(hits.astype(jnp.float32), axis=1)
    earlier = jnp.tril(jnp.ones((sequences, sequences), jnp.float32), -1)
    ranking = jnp.dot(earlier, named)
    weight_of = jnp.sum(jnp.where(hits, chosen_expert_weight[:, :, None], 0.0), axis=1)
    slots = [(ranking == c) & (named > 0) for c in range(CAPACITY)]
    dispatch = jnp.concatenate([s.astype(jnp.bfloat16) for s in slots], axis=1)
    combine = jnp.concatenate([jnp.where(s, weight_of, 0.0) for s in slots], axis=1)

    flat_state = state.reshape(sequences, head_columns, state.shape[3])
    *head_terms, decay, removed, along, value, blended = local_call(
        attention_kernel,
        "attention",
        [bfloat16(sequences, own_columns)] * 4 + [float32(sequences, head_columns)] * 5,
        16,
        [
            pltpu.VMEM((8 * sequences, 128), jnp.float32),
            pltpu.VMEM((2, 8 * sequences, 128), jnp.float32),
            pltpu.VMEM(output_weight.shape, output_weight.dtype),
            pltpu.VMEM(flat_state.shape, flat_state.dtype),
            pltpu.SemaphoreType.DMA((2,)),
        ],
        left=2,
    )(at, *row_pieces, *needed, output_weight, flat_state)
    arrived = scattered(head_terms)
    residual = tokens.astype(jnp.float32) + sum(a.astype(jnp.float32) for a in arrived)

    outgoing = lax.dot_general(
        dispatch,
        residual.astype(jnp.bfloat16),
        (((0,), (0,)), ((), ())),
        preferred_element_type=jnp.float32,
    ).astype(jnp.bfloat16)
    outgoing = outgoing.reshape(CAPACITY, experts, own_columns)
    high = combine.astype(jnp.bfloat16)
    low = (combine - high.astype(jnp.float32)).astype(jnp.bfloat16)
    outgoing, high, low = lax.optimization_barrier((outgoing, high, low))
    came = lax.all_to_all(outgoing, "ep", split_axis=1, concat_axis=1, tiled=True)
    came, decay, removed, along, value, blended = lax.optimization_barrier(
        (came, decay, removed, along, value, blended)
    )
    own_rows = came.reshape(CAPACITY * experts, own_columns)
    row_pieces = gathered(own_rows)
    by_heads = lambda value: value.reshape(state.shape[:3])
    new_state = (
        state * by_heads(decay)[:, :, None, :]
        - by_heads(along)[..., None] * by_heads(removed)[:, :, None, :]
        + by_heads(value)[..., None] * by_heads(blended)[:, :, None, :]
    )
    new_state, *row_pieces = lax.optimization_barrier((new_state, *row_pieces))
    activation = local_call(
        hidden_kernel, "hidden", bfloat16(own_rows.shape[0], expert_gate_weight.shape[2]), 12
    )(
        at,
        *row_pieces,
        vector(second_norm_gain),
        expert_gate_weight[0],
        expert_up_weight[0],
    )
    down_terms = local_call(
        down_kernel, "down", [bfloat16(own_rows.shape[0], own_columns)] * 4, 8
    )(at, activation, expert_down_weight[0])
    arrived = scattered(down_terms)
    shares = sum(a.astype(jnp.float32) for a in arrived).astype(jnp.bfloat16)
    shares = shares.reshape(CAPACITY, experts, own_columns)
    returned = lax.all_to_all(shares, "ep", split_axis=1, concat_axis=1, tiled=True)
    returned = returned.reshape(CAPACITY * experts, own_columns)
    weighted = jnp.dot(
        jnp.concatenate([high, low], axis=0), returned, preferred_element_type=jnp.float32
    )
    layer_out = (residual + weighted[:sequences] + weighted[sequences:]).astype(jnp.bfloat16)
    return (layer_out, new_state)


def solution(mesh):
    in_specs = (
        P("ep", "tp"),
        P("ep", "tp"),
        P(),
        P(),
        P(None, "tp"),
        P(None, "tp"),
        P(None, "tp"),
        P(),
        P(),
        P("tp"),
        P(),
        P(),
        P("tp"),
        P("tp"),
        P("tp", None),
        P("tp"),
        P("tp", None),
        P("ep", "tp", None, None),
        P(),
        P("ep", None),
        P("ep", None),
        P("ep", None, "tp"),
        P("ep", None, "tp"),
        P("ep", "tp", None),
    )
    out_specs = (P("ep", "tp"), P("ep", "tp", None, None))
    return jax.shard_map(shards, mesh=mesh, in_specs=in_specs, out_specs=out_specs, check_vma=False)
```

```python
import math

import jax
import jax.numpy as jnp
from jax import lax
from jax.experimental import pallas as pl
from jax.experimental.pallas import tpu as pltpu
from jax.sharding import PartitionSpec as P


NORM_EPS = 1e-06
GROUP_EPS = 0.00064
KEY_EPS = 1e-06
GATE_LIMIT = 7.0
GATE_SLOPE = 1.702
CAPACITY = 3
HALF_DECAY = math.exp(-0.5)
MIB = 1 << 20


def from_offset(value, offset):
    devices = lax.axis_size("tp")
    return lax.ppermute(value, "tp", [(i, (i - offset) % devices) for i in range(devices)])


def gathered(value):
    pieces = {k: from_offset(value, k) for k in (2, 3, 1)}
    return [value, pieces[1], pieces[2], pieces[3]]


def scattered(values):
    pieces = {k: from_offset(values[k], -k) for k in (2, 1, 3)}
    return [values[0], pieces[1], pieces[2], pieces[3]]


def head_sums(values, same_head):
    high = values.astype(jnp.bfloat16)
    low = (values - high.astype(jnp.float32)).astype(jnp.bfloat16)
    return jnp.dot(high, same_head, preferred_element_type=jnp.float32) + jnp.dot(
        low, same_head, preferred_element_type=jnp.float32
    )


def attention_kernel(
    at,
    p0,
    p1,
    p2,
    p3,
    first_gain,
    share,
    receptance_weight,
    key_weight,
    value_weight,
    decay_down,
    decay_up,
    decay_offset,
    strength_down,
    strength_up,
    removal_scale,
    damping,
    self_weight,
    head_gain,
    state_head,
    output_weight_hbm,
    state_hbm,
    o0,
    o1,
    o2,
    o3,
    decay_out,
    along_out,
    value_out,
    removal_out,
    blended_out,
    vectors,
    results,
    output_weight,
    state_tail,
    sems,
):
    half = state_tail.shape[0]
    state_copy = pltpu.make_async_copy(state_hbm.at[pl.ds(half, half)], state_tail, sems.at[0])
    state_copy.start()
    weight_copy = pltpu.make_async_copy(output_weight_hbm, output_weight, sems.at[1])
    weight_copy.start()
    sequences, columns = along_out.shape
    heads, width = self_weight.shape
    block = p0.shape[1]
    places = [pl.multiple_of(lax.rem(at[0] + k, 4) * block, block) for k in range(4)]
    present = [p[:sequences, :].astype(jnp.float32) for p in (p0, p1, p2, p3)]
    prior = [p[sequences:, :].astype(jnp.float32) for p in (p0, p1, p2, p3)]
    squares = sum(jnp.sum(x * x, axis=1, keepdims=True) for x in present)
    scale = lax.rsqrt(squares / (4 * block) + NORM_EPS)
    weights = (receptance_weight, key_weight, value_weight, decay_down, strength_down)
    sums = [None] * 5
    for place, x, b in zip(places, present, prior):
        rows = pl.ds(place, block)
        normed = x * scale * first_gain[:, rows]
        change = b - normed
        for m, weight in enumerate(weights):
            moved = (normed + change * share[m : m + 1, rows]).astype(jnp.bfloat16)
            part = jnp.dot(moved, weight[rows, :], preferred_element_type=jnp.float32)
            sums[m] = part if sums[m] is None else sums[m] + part
    receptance, key, value, decay_low, strength_low = sums
    own = pl.ds(pl.multiple_of(at[0] * columns, columns), columns)
    decay_pre = decay_offset[...] + jnp.dot(
        jnp.tanh(decay_low).astype(jnp.bfloat16),
        decay_up[:, own],
        preferred_element_type=jnp.float32,
    )
    decay = jnp.exp(-HALF_DECAY * jax.nn.sigmoid(decay_pre))
    alpha = jax.nn.sigmoid(
        jnp.dot(
            strength_low.astype(jnp.bfloat16),
            strength_up[:, own],
            preferred_element_type=jnp.float32,
        )
    )
    lane = lax.broadcasted_iota(jnp.int32, (columns, columns), 1) // width
    row = lax.broadcasted_iota(jnp.int32, (columns, columns), 0) // width
    same_head = (lane == row).astype(jnp.bfloat16)
    removal = key * removal_scale[...]
    removal = removal * lax.rsqrt(head_sums(removal * removal, same_head) + KEY_EPS)
    blended = key * (1.0 + (alpha - 1.0) * damping[...])
    removed = removal * alpha
    pair = 2 * width
    rows_each = 2 * heads

    def of_head(vector, h):
        two = vector[:, h // 2 * pair : h // 2 * pair + pair]
        return pltpu.roll(two, width, 1) if h % 2 else two

    for v, vector in enumerate((removal, decay * receptance)):
        for h in range(heads):
            vectors[pl.ds(v * heads + h, sequences, stride=rows_each), :] = of_head(vector, h)
    for s in range(sequences):
        if s == half:
            state_copy.wait()
        state = state_head if s < half else state_tail
        rows = pl.ds(s * rows_each, rows_each)
        found = lax.dot_general(
            vectors[rows, :][:, :width].astype(jnp.bfloat16),
            state[s % half].astype(jnp.bfloat16),
            (((1,), (1,)), ((), ())),
            preferred_element_type=jnp.float32,
        )
        for c in range(heads // 2):
            results[c, rows, :] = found[:, c * pair : (c + 1) * pair]
    first_of_two = lax.broadcasted_iota(jnp.int32, (sequences, pair), 1) < width

    def of_vector(v):
        parts = []
        for c in range(heads // 2):
            one, other = (
                results[c, pl.ds(v * heads + 2 * c + i, sequences, stride=rows_each), :]
                for i in (0, 1)
            )
            parts.append(jnp.where(first_of_two, one, other))
        return jnp.concatenate(parts, axis=1)

    along, kept = of_vector(0), of_vector(1)
    gains = jnp.concatenate([self_weight[h : h + 1, :] for h in range(heads)], axis=1)
    readout = (
        kept
        - along * head_sums(removed * receptance, same_head)
        + value * head_sums(blended * receptance, same_head)
    )
    centered = readout - head_sums(readout, same_head) / width
    variance = head_sums(centered * centered, same_head) / width
    mixed = (
        centered * lax.rsqrt(variance + GROUP_EPS) * head_gain[...]
        + head_sums(receptance * blended * gains, same_head) * value
    ).astype(jnp.bfloat16)
    weight_copy.wait()
    for place, o in zip(places, (o0, o1, o2, o3)):
        o[...] = jnp.dot(
            mixed, output_weight[:, pl.ds(place, block)], preferred_element_type=jnp.float32
        ).astype(jnp.bfloat16)
    along_out[...] = along
    value_out[...] = value
    for out, vector in ((decay_out, decay), (removal_out, removed), (blended_out, blended)):
        for h in range(heads):
            out[pl.ds(h, sequences, stride=heads), :] = of_head(vector, h)


def renew_kernel(
    decay, removed, blended, along, value, state_hbm, new_state_hbm, state, new_state, sems
):
    sequences, columns, width = state.shape
    heads = columns // width
    groups = sems.shape[1]
    each = sequences // groups

    def copies_of(g):
        part = pl.ds(g * each, each)
        return (
            pltpu.make_async_copy(state_hbm.at[part], state.at[part], sems.at[0, g]),
            pltpu.make_async_copy(new_state.at[part], new_state_hbm.at[part], sems.at[1, g]),
        )

    copies = [copies_of(g) for g in range(groups)]
    for arriving, _ in copies:
        arriving.start()
    along_columns, value_columns = along[...].T, value[...].T
    for g, (arriving, leaving) in enumerate(copies):
        arriving.wait()
        for s in range(g * each, (g + 1) * each):
            for h in range(heads):
                rows = slice(h * width, (h + 1) * width)
                at = slice(s * heads + h, s * heads + h + 1)
                new_state[s, rows, :] = (
                    state[s, rows, :] * decay[at, :width]
                    - along_columns[rows, s : s + 1] * removed[at, :width]
                    + value_columns[rows, s : s + 1] * blended[at, :width]
                )
        leaving.start()
    for _, leaving in copies:
        leaving.wait()


def stack_kernel(first, second, out, sems):
    height = first.shape[0]
    copies = [
        pltpu.make_async_copy(first, out.at[pl.ds(0, height)], sems.at[0]),
        pltpu.make_async_copy(second, out.at[pl.ds(height, height)], sems.at[1]),
    ]
    for copy in copies:
        copy.start()
    for copy in copies:
        copy.wait()


def fetch_kernel(at, *refs):
    sems = refs[-1]
    count = len(sems) - 3
    *sources, down_weight = refs[: count + 1]
    wholes, columns = refs[count + 1 : 2 * count + 1], refs[2 * count + 1 : -1]
    sources[-1] = sources[-1].at[pl.ds(0, wholes[-1].shape[0])]
    copies = [
        pltpu.make_async_copy(source, whole, sems.at[i])
        for i, (source, whole) in enumerate(zip(sources, wholes))
    ]
    for k, piece in enumerate(columns, 1):
        block = piece.shape[1]
        place = pl.multiple_of(lax.rem(at[0] + k, 4) * block, block)
        copies.append(
            pltpu.make_async_copy(
                down_weight.at[:, pl.ds(place, block)], piece, sems.at[count + k - 1]
            )
        )
    for copy in copies:
        copy.start()
    for copy in copies:
        copy.wait()


def hidden_kernel(at, x0, x1, x2, x2_rest, x3, gain, gate_weight, up_weight, out):
    pieces = (x0[...], x1[...], jnp.concatenate([x2[...], x2_rest[...]], axis=0), x3[...])
    width = x0.shape[1]
    places = [lax.rem(at[0] + k, 4) * width for k in range(4)]
    floats = [x.astype(jnp.float32) for x in pieces]
    squares = sum(jnp.sum(f * f, axis=1, keepdims=True) for f in floats)
    scale = lax.rsqrt(squares / (4 * width) + NORM_EPS)
    gate = jnp.zeros(out.shape, jnp.float32)
    up = jnp.zeros(out.shape, jnp.float32)
    for f, place in zip(floats, places):
        rows = pl.ds(pl.multiple_of(place, width), width)
        x = (f * scale * gain[:, rows]).astype(jnp.bfloat16)
        gate = gate + jnp.dot(x, gate_weight[rows, :], preferred_element_type=jnp.float32)
        up = up + jnp.dot(x, up_weight[rows, :], preferred_element_type=jnp.float32)
    gate = jnp.minimum(gate, GATE_LIMIT)
    up = jnp.clip(up, -GATE_LIMIT, GATE_LIMIT)
    out[...] = ((up + 1.0) * gate * jax.nn.sigmoid(GATE_SLOPE * gate)).astype(jnp.bfloat16)


def down_kernel(at, a0, a1, a2, a3, w1, w2, w3, down_weight, out):
    block = out.shape[1]
    own = pl.ds(pl.multiple_of(at[0] * block, block), block)
    total = jnp.dot(a0[...], down_weight[:, own], preferred_element_type=jnp.float32)
    for a, w in ((a1, w1), (a2, w2), (a3, w3)):
        total = total + jnp.dot(a[...], w[...], preferred_element_type=jnp.float32)
    out[...] = total.astype(jnp.bfloat16)


def local_call(kernel, shapes, limit, scratch=(), scalars=0, left=0):
    def call(*operands):
        in_vmem = pl.BlockSpec(memory_space=pltpu.VMEM)
        count = len(operands) - left
        operands = operands[:count] + tuple(
            pltpu.with_memory_space_constraint(value, pltpu.HBM) for value in operands[count:]
        )
        return pl.pallas_call(
            kernel,
            out_shape=shapes,
            in_specs=[pl.BlockSpec(memory_space=pltpu.SMEM)] * scalars
            + [in_vmem] * (count - scalars)
            + [pl.BlockSpec(memory_space=pltpu.HBM)] * left,
            out_specs=jax.tree.map(lambda _: in_vmem, shapes),
            scratch_shapes=scratch,
            compiler_params=pltpu.CompilerParams(vmem_limit_bytes=limit * MIB),
        )(*operands)

    return call


def shards(
    tokens,
    previous,
    first_norm_gain,
    token_shift_share,
    receptance_weight,
    key_weight,
    value_weight,
    decay_down_map,
    decay_up_map,
    decay_offset,
    strength_down_map,
    strength_up_map,
    removal_key_scale,
    key_damping,
    self_term_weight,
    head_norm_gain,
    output_weight,
    state,
    second_norm_gain,
    routes,
    chosen_expert_weight,
    expert_gate_weight,
    expert_up_weight,
    expert_down_weight,
):
    at = lax.axis_index("tp")[None]
    sequences, own_columns = tokens.shape
    head_columns = receptance_weight.shape[1]
    float32 = lambda *shape: jax.ShapeDtypeStruct(shape, jnp.float32)
    bfloat16 = lambda *shape: jax.ShapeDtypeStruct(shape, jnp.bfloat16)
    both = local_call(
        stack_kernel,
        jax.ShapeDtypeStruct((2 * sequences, own_columns), tokens.dtype),
        1,
        [pltpu.SemaphoreType.DMA((2,))],
        left=2,
    )(tokens, previous)
    row_pieces = gathered(both)

    vector = lambda value: value[None, :]
    needed = (
        vector(first_norm_gain),
        token_shift_share,
        receptance_weight,
        key_weight,
        value_weight,
        decay_down_map,
        decay_up_map,
        vector(decay_offset),
        strength_down_map,
        strength_up_map,
        vector(removal_key_scale),
        vector(key_damping),
        self_term_weight,
        vector(head_norm_gain),
    )
    flat_state = state.reshape(sequences, head_columns, state.shape[3])
    shapes = [jax.ShapeDtypeStruct(a.shape, a.dtype) for a in needed]
    shapes.append(float32(sequences // 2, *flat_state.shape[1:]))
    *needed, down_1, down_2, down_3 = local_call(
        fetch_kernel,
        shapes + [bfloat16(expert_down_weight.shape[1], own_columns)] * 3,
        14,
        [pltpu.SemaphoreType.DMA((len(shapes) + 3,))],
        scalars=1,
        left=len(shapes) + 1,
    )(at, *needed, flat_state, expert_down_weight[0])

    experts = expert_gate_weight.shape[0] * lax.axis_size("ep")
    ids = jnp.arange(experts, dtype=jnp.int32)
    hits = routes[:, :, None] == ids[None, None, :]
    named = jnp.sum(hits.astype(jnp.float32), axis=1)
    earlier = jnp.tril(jnp.ones((sequences, sequences), jnp.float32), -1)
    ranking = jnp.dot(earlier, named)
    weight_of = jnp.sum(jnp.where(hits, chosen_expert_weight[:, :, None], 0.0), axis=1)
    slots = [(ranking == c) & (named > 0) for c in range(CAPACITY)]
    dispatch = jnp.concatenate([s.astype(jnp.bfloat16) for s in slots], axis=1)
    combine = jnp.concatenate([jnp.where(s, weight_of, 0.0) for s in slots], axis=1)

    *head_terms, decay, along, value, removed, blended = local_call(
        attention_kernel,
        [bfloat16(sequences, own_columns)] * 4
        + [float32(sequences * state.shape[1], 128)]
        + [float32(sequences, head_columns)] * 2
        + [float32(sequences * state.shape[1], 128)] * 2,
        16,
        [
            pltpu.VMEM((8 * sequences, 128), jnp.float32),
            pltpu.VMEM((2, 8 * sequences, 128), jnp.float32),
            pltpu.VMEM(output_weight.shape, output_weight.dtype),
            pltpu.VMEM((sequences // 2, *flat_state.shape[1:]), jnp.float32),
            pltpu.SemaphoreType.DMA((2,)),
        ],
        scalars=1,
        left=2,
    )(at, *row_pieces, *needed, output_weight, flat_state)
    arrived = scattered(head_terms)
    down_pieces = scattered([None, down_1, down_2, down_3])[1:]
    residual = tokens.astype(jnp.float32) + sum(a.astype(jnp.float32) for a in arrived)

    outgoing = lax.dot_general(
        dispatch,
        residual.astype(jnp.bfloat16),
        (((0,), (0,)), ((), ())),
        preferred_element_type=jnp.float32,
    ).astype(jnp.bfloat16)
    outgoing = outgoing.reshape(CAPACITY, experts, own_columns)
    high = combine.astype(jnp.bfloat16)
    low = (combine - high.astype(jnp.float32)).astype(jnp.bfloat16)
    outgoing, high, low = lax.optimization_barrier((outgoing, high, low))
    came = lax.all_to_all(outgoing, "ep", split_axis=1, concat_axis=1, tiled=True)
    own_rows = came.reshape(CAPACITY * experts, own_columns)
    half = own_rows.shape[0] // 2
    second = from_offset(own_rows[:half], 2)
    first = from_offset(own_rows, 1)
    third = from_offset(own_rows, 3)
    second_rest = from_offset(first[half:], 1)
    activation = local_call(
        hidden_kernel, bfloat16(own_rows.shape[0], expert_gate_weight.shape[2]), 12, scalars=1
    )(
        at,
        own_rows,
        first,
        second,
        second_rest,
        third,
        vector(second_norm_gain),
        expert_gate_weight[0],
        expert_up_weight[0],
    )
    activation, *renewing = lax.optimization_barrier(
        (activation, decay, removed, blended, along, value)
    )
    act_pieces = scattered([activation] * 4)
    new_state = pl.pallas_call(
        renew_kernel,
        out_shape=float32(*flat_state.shape),
        in_specs=[pl.BlockSpec(memory_space=pltpu.VMEM)] * 5
        + [pl.BlockSpec(memory_space=pltpu.HBM)],
        out_specs=pl.BlockSpec(memory_space=pltpu.HBM),
        scratch_shapes=[
            pltpu.VMEM(flat_state.shape, jnp.float32),
            pltpu.VMEM(flat_state.shape, jnp.float32),
            pltpu.SemaphoreType.DMA((2, 8)),
        ],
        compiler_params=pltpu.CompilerParams(vmem_limit_bytes=12 * MIB),
        name="renew",
    )(*renewing, pltpu.with_memory_space_constraint(flat_state, pltpu.HBM))
    new_state, *act_pieces = lax.optimization_barrier((new_state, *act_pieces))
    new_state = new_state.reshape(state.shape)
    shares = local_call(
        down_kernel, bfloat16(own_rows.shape[0], own_columns), 8, scalars=1
    )(at, *act_pieces, *down_pieces, expert_down_weight[0])
    shares = shares.reshape(CAPACITY, experts, own_columns)
    returned = lax.all_to_all(shares, "ep", split_axis=1, concat_axis=1, tiled=True)
    returned = returned.reshape(CAPACITY * experts, own_columns)
    weighted = jnp.dot(
        jnp.concatenate([high, low], axis=0), returned, preferred_element_type=jnp.float32
    )
    layer_out = (residual + weighted[:sequences] + weighted[sequences:]).astype(jnp.bfloat16)
    return (layer_out, new_state)


def solution(mesh):
    in_specs = (
        P("ep", "tp"),
        P("ep", "tp"),
        P(),
        P(),
        P(None, "tp"),
        P(None, "tp"),
        P(None, "tp"),
        P(),
        P(),
        P("tp"),
        P(),
        P(),
        P("tp"),
        P("tp"),
        P("tp", None),
        P("tp"),
        P("tp", None),
        P("ep", "tp", None, None),
        P(),
        P("ep", None),
        P("ep", None),
        P("ep", None, "tp"),
        P("ep", None, "tp"),
        P("ep", "tp", None),
    )
    out_specs = (P("ep", "tp"), P("ep", "tp", None, None))

    return jax.shard_map(shards, mesh=mesh, in_specs=in_specs, out_specs=out_specs, check_vma=False)
```

```python
import math

import jax
import jax.numpy as jnp
from jax import lax
from jax.experimental import pallas as pl
from jax.experimental.pallas import tpu as pltpu
from jax.sharding import PartitionSpec as P


NORM_EPS = 1e-06
GROUP_EPS = 0.00064
KEY_EPS = 1e-06
GATE_LIMIT = 7.0
GATE_SLOPE = 1.702
CAPACITY = 3
HALF_DECAY = math.exp(-0.5)
MIB = 1 << 20


def from_offset(value, offset):
    devices = lax.axis_size("tp")
    return lax.ppermute(value, "tp", [(i, (i - offset) % devices) for i in range(devices)])


def gathered(value):
    pieces = {k: from_offset(value, k) for k in (2, 3, 1)}
    return [value, pieces[1], pieces[2], pieces[3]]


def scattered(values):
    pieces = {k: from_offset(values[k], -k) for k in (2, 1, 3)}
    return [values[0], pieces[1], pieces[2], pieces[3]]


def head_sums(values, same_head):
    high = values.astype(jnp.bfloat16)
    low = (values - high.astype(jnp.float32)).astype(jnp.bfloat16)
    return jnp.dot(high, same_head, preferred_element_type=jnp.float32) + jnp.dot(
        low, same_head, preferred_element_type=jnp.float32
    )


def attention_kernel(
    at,
    p0,
    p1,
    p2,
    p3,
    first_gain,
    share,
    receptance_weight,
    key_weight,
    value_weight,
    decay_down,
    decay_up,
    decay_offset,
    strength_down,
    strength_up,
    removal_scale,
    damping,
    self_weight,
    head_gain,
    output_weight,
    state,
    o0,
    o1,
    o2,
    o3,
    decay_out,
    along_out,
    value_out,
    removal_out,
    blended_out,
    vectors,
    results,
):
    sequences, columns = along_out.shape
    heads, width = self_weight.shape
    block = p0.shape[1]
    places = [pl.multiple_of(lax.rem(at[0] + k, 4) * block, block) for k in range(4)]
    present = [p[:sequences, :].astype(jnp.float32) for p in (p0, p1, p2, p3)]
    prior = [p[sequences:, :].astype(jnp.float32) for p in (p0, p1, p2, p3)]
    squares = sum(jnp.sum(x * x, axis=1, keepdims=True) for x in present)
    scale = lax.rsqrt(squares / (4 * block) + NORM_EPS)
    weights = (receptance_weight, key_weight, value_weight, decay_down, strength_down)
    sums = [None] * 5
    for place, x, b in zip(places, present, prior):
        rows = pl.ds(place, block)
        normed = x * scale * first_gain[:, rows]
        change = b - normed
        for m, weight in enumerate(weights):
            moved = (normed + change * share[m : m + 1, rows]).astype(jnp.bfloat16)
            part = jnp.dot(moved, weight[rows, :], preferred_element_type=jnp.float32)
            sums[m] = part if sums[m] is None else sums[m] + part
    receptance, key, value, decay_low, strength_low = sums
    own = pl.ds(pl.multiple_of(at[0] * columns, columns), columns)
    decay_pre = decay_offset[...] + jnp.dot(
        jnp.tanh(decay_low).astype(jnp.bfloat16),
        decay_up[:, own],
        preferred_element_type=jnp.float32,
    )
    decay = jnp.exp(-HALF_DECAY * jax.nn.sigmoid(decay_pre))
    alpha = jax.nn.sigmoid(
        jnp.dot(
            strength_low.astype(jnp.bfloat16),
            strength_up[:, own],
            preferred_element_type=jnp.float32,
        )
    )
    lane = lax.broadcasted_iota(jnp.int32, (columns, columns), 1) // width
    row = lax.broadcasted_iota(jnp.int32, (columns, columns), 0) // width
    same_head = (lane == row).astype(jnp.bfloat16)
    removal = key * removal_scale[...]
    removal = removal * lax.rsqrt(head_sums(removal * removal, same_head) + KEY_EPS)
    blended = key * (1.0 + (alpha - 1.0) * damping[...])
    removed = removal * alpha
    pair = 2 * width
    rows_each = 2 * heads

    def of_head(vector, h):
        two = vector[:, h // 2 * pair : h // 2 * pair + pair]
        return pltpu.roll(two, width, 1) if h % 2 else two

    for v, vector in enumerate((removal, decay * receptance)):
        for h in range(heads):
            vectors[pl.ds(v * heads + h, sequences, stride=rows_each), :] = of_head(vector, h)
    for s in range(sequences):
        rows = pl.ds(s * rows_each, rows_each)
        found = lax.dot_general(
            vectors[rows, :][:, :width].astype(jnp.bfloat16),
            state[s].astype(jnp.bfloat16),
            (((1,), (1,)), ((), ())),
            preferred_element_type=jnp.float32,
        )
        for c in range(heads // 2):
            results[c, rows, :] = found[:, c * pair : (c + 1) * pair]
    first_of_two = lax.broadcasted_iota(jnp.int32, (sequences, pair), 1) < width

    def of_vector(v):
        parts = []
        for c in range(heads // 2):
            one, other = (
                results[c, pl.ds(v * heads + 2 * c + i, sequences, stride=rows_each), :]
                for i in (0, 1)
            )
            parts.append(jnp.where(first_of_two, one, other))
        return jnp.concatenate(parts, axis=1)

    along, kept = of_vector(0), of_vector(1)
    gains = jnp.concatenate([self_weight[h : h + 1, :] for h in range(heads)], axis=1)
    readout = (
        kept
        - along * head_sums(removed * receptance, same_head)
        + value * head_sums(blended * receptance, same_head)
    )
    centered = readout - head_sums(readout, same_head) / width
    variance = head_sums(centered * centered, same_head) / width
    mixed = (
        centered * lax.rsqrt(variance + GROUP_EPS) * head_gain[...]
        + head_sums(receptance * blended * gains, same_head) * value
    ).astype(jnp.bfloat16)
    for place, o in zip(places, (o0, o1, o2, o3)):
        o[...] = jnp.dot(
            mixed, output_weight[:, pl.ds(place, block)], preferred_element_type=jnp.float32
        ).astype(jnp.bfloat16)
    along_out[...] = along
    value_out[...] = value
    for out, vector in ((decay_out, decay), (removal_out, removed), (blended_out, blended)):
        for h in range(heads):
            out[pl.ds(h, sequences, stride=heads), :] = of_head(vector, h)


def renew_kernel(
    decay, removed, blended, along, value, state_hbm, new_state_hbm, state, new_state, sems
):
    sequences, columns, width = state.shape
    heads = columns // width
    groups = sems.shape[1]
    each = sequences // groups

    def copies_of(g):
        part = pl.ds(g * each, each)
        return (
            pltpu.make_async_copy(state_hbm.at[part], state.at[part], sems.at[0, g]),
            pltpu.make_async_copy(new_state.at[part], new_state_hbm.at[part], sems.at[1, g]),
        )

    copies = [copies_of(g) for g in range(groups)]
    for arriving, _ in copies:
        arriving.start()
    along_columns, value_columns = along[...].T, value[...].T
    for g, (arriving, leaving) in enumerate(copies):
        arriving.wait()
        for s in range(g * each, (g + 1) * each):
            for h in range(heads):
                rows = slice(h * width, (h + 1) * width)
                at = slice(s * heads + h, s * heads + h + 1)
                new_state[s, rows, :] = (
                    state[s, rows, :] * decay[at, :width]
                    - along_columns[rows, s : s + 1] * removed[at, :width]
                    + value_columns[rows, s : s + 1] * blended[at, :width]
                )
        leaving.start()
    for _, leaving in copies:
        leaving.wait()


def stack_kernel(first, second, out, sems):
    height = first.shape[0]
    copies = [
        pltpu.make_async_copy(first, out.at[pl.ds(0, height)], sems.at[0]),
        pltpu.make_async_copy(second, out.at[pl.ds(height, height)], sems.at[1]),
    ]
    for copy in copies:
        copy.start()
    for copy in copies:
        copy.wait()


def route_kernel(
    at,
    routes_hbm,
    weights_hbm,
    down_weight,
    dispatch,
    high,
    low,
    piece_1,
    piece_2,
    piece_3,
    routes,
    weights,
    sems,
):
    needed = [
        pltpu.make_async_copy(routes_hbm, routes, sems.at[3]),
        pltpu.make_async_copy(weights_hbm, weights, sems.at[4]),
    ]
    for copy in needed:
        copy.start()
    copies = []
    for k, piece in enumerate((piece_1, piece_2, piece_3), 1):
        block = piece.shape[1]
        place = pl.multiple_of(lax.rem(at[0] + k, 4) * block, block)
        copies.append(
            pltpu.make_async_copy(down_weight.at[:, pl.ds(place, block)], piece, sems.at[k - 1])
        )
    for copy in copies:
        copy.start()
    for copy in needed:
        copy.wait()
    choices, sequences = routes.shape
    experts = dispatch.shape[0] // CAPACITY
    ids = lax.broadcasted_iota(jnp.int32, (experts, sequences), 0)
    named = jnp.zeros((experts, sequences), jnp.float32)
    weight = jnp.zeros((experts, sequences), jnp.float32)
    for c in range(choices):
        hit = ids == routes[c : c + 1, :]
        named = jnp.where(hit, 1.0, named)
        weight = jnp.where(hit, weights[c : c + 1, :], weight)
    row = lax.broadcasted_iota(jnp.int32, (sequences, sequences), 0)
    column = lax.broadcasted_iota(jnp.int32, (sequences, sequences), 1)
    earlier = (row < column).astype(jnp.bfloat16)
    ranking = jnp.dot(named.astype(jnp.bfloat16), earlier, preferred_element_type=jnp.float32)
    for c in range(CAPACITY):
        rows = slice(c * experts, (c + 1) * experts)
        here = jnp.where(ranking == c, named, 0.0)
        dispatch[rows, :] = here.astype(jnp.bfloat16)
        share = here * weight
        first = share.astype(jnp.bfloat16)
        high[rows, :] = first
        low[rows, :] = (share - first.astype(jnp.float32)).astype(jnp.bfloat16)
    for copy in copies:
        copy.wait()


def hidden_kernel(at, x0, x1, x2, x3, gain, gate_weight, up_weight, out):
    pieces = (x0[...], x1[...], x2[...], x3[...])
    width = x0.shape[1]
    places = [lax.rem(at[0] + k, 4) * width for k in range(4)]
    floats = [x.astype(jnp.float32) for x in pieces]
    squares = sum(jnp.sum(f * f, axis=1, keepdims=True) for f in floats)
    scale = lax.rsqrt(squares / (4 * width) + NORM_EPS)
    gate = jnp.zeros(out.shape, jnp.float32)
    up = jnp.zeros(out.shape, jnp.float32)
    for f, place in zip(floats, places):
        rows = pl.ds(pl.multiple_of(place, width), width)
        x = (f * scale * gain[:, rows]).astype(jnp.bfloat16)
        gate = gate + jnp.dot(x, gate_weight[rows, :], preferred_element_type=jnp.float32)
        up = up + jnp.dot(x, up_weight[rows, :], preferred_element_type=jnp.float32)
    gate = jnp.minimum(gate, GATE_LIMIT)
    up = jnp.clip(up, -GATE_LIMIT, GATE_LIMIT)
    out[...] = ((up + 1.0) * gate * jax.nn.sigmoid(GATE_SLOPE * gate)).astype(jnp.bfloat16)


def down_kernel(at, a0, a1, a2, a3, w1, w2, w3, down_weight, out):
    block = out.shape[1]
    own = pl.ds(pl.multiple_of(at[0] * block, block), block)
    total = jnp.dot(a0[...], down_weight[:, own], preferred_element_type=jnp.float32)
    for a, w in ((a1, w1), (a2, w2), (a3, w3)):
        total = total + jnp.dot(a[...], w[...], preferred_element_type=jnp.float32)
    out[...] = total.astype(jnp.bfloat16)


def local_call(kernel, shapes, limit, scratch=(), scalars=0, left=0, cost=None):
    def call(*operands):
        in_vmem = pl.BlockSpec(memory_space=pltpu.VMEM)
        count = len(operands) - left
        operands = operands[:count] + tuple(
            pltpu.with_memory_space_constraint(value, pltpu.HBM) for value in operands[count:]
        )
        return pl.pallas_call(
            kernel,
            out_shape=shapes,
            in_specs=[pl.BlockSpec(memory_space=pltpu.SMEM)] * scalars
            + [in_vmem] * (count - scalars)
            + [pl.BlockSpec(memory_space=pltpu.HBM)] * left,
            out_specs=jax.tree.map(lambda _: in_vmem, shapes),
            scratch_shapes=scratch,
            compiler_params=pltpu.CompilerParams(vmem_limit_bytes=limit * MIB),
            cost_estimate=cost,
        )(*operands)

    return call


def shards(
    tokens,
    previous,
    first_norm_gain,
    token_shift_share,
    receptance_weight,
    key_weight,
    value_weight,
    decay_down_map,
    decay_up_map,
    decay_offset,
    strength_down_map,
    strength_up_map,
    removal_key_scale,
    key_damping,
    self_term_weight,
    head_norm_gain,
    output_weight,
    state,
    second_norm_gain,
    routes,
    chosen_expert_weight,
    expert_gate_weight,
    expert_up_weight,
    expert_down_weight,
):
    at = lax.axis_index("tp")[None]
    sequences, own_columns = tokens.shape
    head_columns = receptance_weight.shape[1]
    float32 = lambda *shape: jax.ShapeDtypeStruct(shape, jnp.float32)
    bfloat16 = lambda *shape: jax.ShapeDtypeStruct(shape, jnp.bfloat16)
    both = local_call(
        stack_kernel,
        jax.ShapeDtypeStruct((2 * sequences, own_columns), tokens.dtype),
        1,
        [pltpu.SemaphoreType.DMA((2,))],
        left=2,
    )(tokens, previous)
    row_pieces = gathered(both)

    vector = lambda value: value[None, :]
    needed = (
        vector(first_norm_gain),
        token_shift_share,
        receptance_weight,
        key_weight,
        value_weight,
        decay_down_map,
        decay_up_map,
        vector(decay_offset),
        strength_down_map,
        strength_up_map,
        vector(removal_key_scale),
        vector(key_damping),
        self_term_weight,
        vector(head_norm_gain),
    )
    flat_state = state.reshape(sequences, head_columns, state.shape[3])
    experts = expert_gate_weight.shape[0] * lax.axis_size("ep")
    slots = CAPACITY * experts
    dispatch, high, low, down_1, down_2, down_3 = local_call(
        route_kernel,
        [bfloat16(slots, sequences)] * 3 + [bfloat16(expert_down_weight.shape[1], own_columns)] * 3,
        4,
        [
            pltpu.VMEM(routes.shape[::-1], routes.dtype),
            pltpu.VMEM(routes.shape[::-1], jnp.float32),
            pltpu.SemaphoreType.DMA((5,)),
        ],
        scalars=1,
        left=3,
        cost=pl.CostEstimate(flops=4_000_000_000, transcendentals=0, bytes_accessed=32_000_000),
    )(at, routes.T, chosen_expert_weight.T, expert_down_weight[0])

    dispatch, high, low, down_1, down_2, down_3, *row_pieces = lax.optimization_barrier(
        (dispatch, high, low, down_1, down_2, down_3, *row_pieces)
    )
    *head_terms, decay, along, value, removed, blended = local_call(
        attention_kernel,
        [bfloat16(sequences, own_columns)] * 4
        + [float32(sequences * state.shape[1], 128)]
        + [float32(sequences, head_columns)] * 2
        + [float32(sequences * state.shape[1], 128)] * 2,
        16,
        [
            pltpu.VMEM((8 * sequences, 128), jnp.float32),
            pltpu.VMEM((2, 8 * sequences, 128), jnp.float32),
        ],
        scalars=1,
    )(at, *row_pieces, *needed, output_weight, flat_state)
    arrived = scattered(head_terms)
    down_pieces = scattered([None, down_1, down_2, down_3])[1:]
    residual = tokens.astype(jnp.float32) + sum(a.astype(jnp.float32) for a in arrived)

    outgoing = jnp.dot(
        dispatch, residual.astype(jnp.bfloat16), preferred_element_type=jnp.float32
    ).astype(jnp.bfloat16)
    outgoing = outgoing.reshape(CAPACITY, experts, own_columns)
    came = lax.all_to_all(outgoing, "ep", split_axis=1, concat_axis=1, tiled=True)
    came, decay, removed, blended, along, value = lax.optimization_barrier(
        (came, decay, removed, blended, along, value)
    )
    own_rows = came.reshape(CAPACITY * experts, own_columns)
    row_pieces = gathered(own_rows)
    new_state = pl.pallas_call(
        renew_kernel,
        out_shape=float32(*flat_state.shape),
        in_specs=[pl.BlockSpec(memory_space=pltpu.VMEM)] * 5
        + [pl.BlockSpec(memory_space=pltpu.HBM)],
        out_specs=pl.BlockSpec(memory_space=pltpu.HBM),
        scratch_shapes=[
            pltpu.VMEM(flat_state.shape, jnp.float32),
            pltpu.VMEM(flat_state.shape, jnp.float32),
            pltpu.SemaphoreType.DMA((2, 8)),
        ],
        compiler_params=pltpu.CompilerParams(vmem_limit_bytes=12 * MIB),
        name="renew",
    )(decay, removed, blended, along, value, pltpu.with_memory_space_constraint(flat_state, pltpu.HBM))
    new_state, *row_pieces = lax.optimization_barrier((new_state, *row_pieces))
    new_state = new_state.reshape(state.shape)
    activation = local_call(
        hidden_kernel, bfloat16(own_rows.shape[0], expert_gate_weight.shape[2]), 12, scalars=1
    )(
        at,
        *row_pieces,
        vector(second_norm_gain),
        expert_gate_weight[0],
        expert_up_weight[0],
    )
    act_pieces = scattered([activation] * 4)
    shares = local_call(
        down_kernel, bfloat16(own_rows.shape[0], own_columns), 8, scalars=1
    )(at, *act_pieces, *down_pieces, expert_down_weight[0])
    shares = shares.reshape(CAPACITY, experts, own_columns)
    returned = lax.all_to_all(shares, "ep", split_axis=1, concat_axis=1, tiled=True)
    returned = returned.reshape(CAPACITY * experts, own_columns)
    weighted = lax.dot_general(
        jnp.concatenate([high, low], axis=1),
        returned,
        (((0,), (0,)), ((), ())),
        preferred_element_type=jnp.float32,
    )
    layer_out = (residual + weighted[:sequences] + weighted[sequences:]).astype(jnp.bfloat16)
    return (layer_out, new_state)


def solution(mesh):
    in_specs = (
        P("ep", "tp"),
        P("ep", "tp"),
        P(),
        P(),
        P(None, "tp"),
        P(None, "tp"),
        P(None, "tp"),
        P(),
        P(),
        P("tp"),
        P(),
        P(),
        P("tp"),
        P("tp"),
        P("tp", None),
        P("tp"),
        P("tp", None),
        P("ep", "tp", None, None),
        P(),
        P("ep", None),
        P("ep", None),
        P("ep", None, "tp"),
        P("ep", None, "tp"),
        P("ep", "tp", None),
    )
    out_specs = (P("ep", "tp"), P("ep", "tp", None, None))

    return jax.shard_map(shards, mesh=mesh, in_specs=in_specs, out_specs=out_specs, check_vma=False)
```

```python
import math

import jax
import jax.numpy as jnp
from jax import lax
from jax.experimental import pallas as pl
from jax.experimental.pallas import tpu as pltpu
from jax.sharding import PartitionSpec as P


NORM_EPS = 1e-06
GROUP_EPS = 0.00064
KEY_EPS = 1e-06
GATE_LIMIT = 7.0
GATE_SLOPE = 1.702
CAPACITY = 3
HALF_DECAY = math.exp(-0.5)
MIB = 1 << 20


def from_offset(value, offset):
    devices = lax.axis_size("tp")
    return lax.ppermute(value, "tp", [(i, (i - offset) % devices) for i in range(devices)])


def gathered(value):
    pieces = {k: from_offset(value, k) for k in (2, 3, 1)}
    return [value, pieces[1], pieces[2], pieces[3]]


def scattered(values):
    pieces = {k: from_offset(values[k], -k) for k in (2, 1, 3)}
    return [values[0], pieces[1], pieces[2], pieces[3]]


def head_sums(values, same_head):
    high = values.astype(jnp.bfloat16)
    low = (values - high.astype(jnp.float32)).astype(jnp.bfloat16)
    return jnp.dot(high, same_head, preferred_element_type=jnp.float32) + jnp.dot(
        low, same_head, preferred_element_type=jnp.float32
    )


def attention_kernel(
    at,
    p0,
    p1,
    p2,
    p3,
    first_gain,
    share,
    receptance_weight,
    key_weight,
    value_weight,
    decay_down,
    decay_up,
    decay_offset,
    strength_down,
    strength_up,
    removal_scale,
    damping,
    self_weight,
    head_gain,
    output_weight,
    state,
    o0,
    o1,
    o2,
    o3,
    decay_out,
    along_out,
    value_out,
    removal_out,
    blended_out,
    vectors,
    results,
):
    sequences, columns = along_out.shape
    heads, width = self_weight.shape
    block = p0.shape[1]
    places = [pl.multiple_of(lax.rem(at[0] + k, 4) * block, block) for k in range(4)]
    present = [p[:sequences, :].astype(jnp.float32) for p in (p0, p1, p2, p3)]
    prior = [p[sequences:, :].astype(jnp.float32) for p in (p0, p1, p2, p3)]
    squares = sum(jnp.sum(x * x, axis=1, keepdims=True) for x in present)
    scale = lax.rsqrt(squares / (4 * block) + NORM_EPS)
    weights = (receptance_weight, key_weight, value_weight, decay_down, strength_down)
    sums = [None] * 5
    for place, x, b in zip(places, present, prior):
        rows = pl.ds(place, block)
        normed = x * scale * first_gain[:, rows]
        change = b - normed
        for m, weight in enumerate(weights):
            moved = (normed + change * share[m : m + 1, rows]).astype(jnp.bfloat16)
            part = jnp.dot(moved, weight[rows, :], preferred_element_type=jnp.float32)
            sums[m] = part if sums[m] is None else sums[m] + part
    receptance, key, value, decay_low, strength_low = sums
    own = pl.ds(pl.multiple_of(at[0] * columns, columns), columns)
    decay_pre = decay_offset[...] + jnp.dot(
        jnp.tanh(decay_low).astype(jnp.bfloat16),
        decay_up[:, own],
        preferred_element_type=jnp.float32,
    )
    decay = jnp.exp(-HALF_DECAY * jax.nn.sigmoid(decay_pre))
    alpha = jax.nn.sigmoid(
        jnp.dot(
            strength_low.astype(jnp.bfloat16),
            strength_up[:, own],
            preferred_element_type=jnp.float32,
        )
    )
    lane = lax.broadcasted_iota(jnp.int32, (columns, columns), 1) // width
    row = lax.broadcasted_iota(jnp.int32, (columns, columns), 0) // width
    same_head = (lane == row).astype(jnp.bfloat16)
    removal = key * removal_scale[...]
    removal = removal * lax.rsqrt(head_sums(removal * removal, same_head) + KEY_EPS)
    blended = key * (1.0 + (alpha - 1.0) * damping[...])
    removed = removal * alpha
    pair = 2 * width
    rows_each = 2 * heads

    def of_head(vector, h):
        two = vector[:, h // 2 * pair : h // 2 * pair + pair]
        return pltpu.roll(two, width, 1) if h % 2 else two

    for v, vector in enumerate((removal, decay * receptance)):
        for h in range(heads):
            vectors[pl.ds(v * heads + h, sequences, stride=rows_each), :] = of_head(vector, h)
    for s in range(sequences):
        rows = pl.ds(s * rows_each, rows_each)
        found = lax.dot_general(
            vectors[rows, :][:, :width].astype(jnp.bfloat16),
            state[s].astype(jnp.bfloat16),
            (((1,), (1,)), ((), ())),
            preferred_element_type=jnp.float32,
        )
        for c in range(heads // 2):
            results[c, rows, :] = found[:, c * pair : (c + 1) * pair]
    first_of_two = lax.broadcasted_iota(jnp.int32, (sequences, pair), 1) < width

    def of_vector(v):
        parts = []
        for c in range(heads // 2):
            one, other = (
                results[c, pl.ds(v * heads + 2 * c + i, sequences, stride=rows_each), :]
                for i in (0, 1)
            )
            parts.append(jnp.where(first_of_two, one, other))
        return jnp.concatenate(parts, axis=1)

    along, kept = of_vector(0), of_vector(1)
    gains = jnp.concatenate([self_weight[h : h + 1, :] for h in range(heads)], axis=1)
    readout = (
        kept
        - along * head_sums(removed * receptance, same_head)
        + value * head_sums(blended * receptance, same_head)
    )
    centered = readout - head_sums(readout, same_head) / width
    variance = head_sums(centered * centered, same_head) / width
    mixed = (
        centered * lax.rsqrt(variance + GROUP_EPS) * head_gain[...]
        + head_sums(receptance * blended * gains, same_head) * value
    ).astype(jnp.bfloat16)
    for k, place in enumerate(places):
        piece = jnp.dot(
            mixed, output_weight[:, pl.ds(place, block)], preferred_element_type=jnp.float32
        ).astype(jnp.bfloat16)
        outs = (o0, o1, o2, o3)
        outs[k][:, :block] = piece
        outs[(k + 2) % 4][:, block:] = piece
    along_out[...] = along
    value_out[...] = value
    for out, vector in ((decay_out, decay), (removal_out, removed), (blended_out, blended)):
        for h in range(heads):
            out[pl.ds(h, sequences, stride=heads), :] = of_head(vector, h)


def renew_kernel(
    decay, removed, blended, along, value, state_hbm, new_state_hbm, state, new_state, sems
):
    sequences, columns, width = state.shape
    heads = columns // width
    groups = sems.shape[1]
    each = sequences // groups

    def copies_of(g):
        part = pl.ds(g * each, each)
        return (
            pltpu.make_async_copy(state_hbm.at[part], state.at[part], sems.at[0, g]),
            pltpu.make_async_copy(new_state.at[part], new_state_hbm.at[part], sems.at[1, g]),
        )

    copies = [copies_of(g) for g in range(groups)]
    for arriving, _ in copies:
        arriving.start()
    along_columns, value_columns = along[...].T, value[...].T
    for g, (arriving, leaving) in enumerate(copies):
        arriving.wait()
        for s in range(g * each, (g + 1) * each):
            for h in range(heads):
                rows = slice(h * width, (h + 1) * width)
                at = slice(s * heads + h, s * heads + h + 1)
                new_state[s, rows, :] = (
                    state[s, rows, :] * decay[at, :width]
                    - along_columns[rows, s : s + 1] * removed[at, :width]
                    + value_columns[rows, s : s + 1] * blended[at, :width]
                )
        leaving.start()
    for _, leaving in copies:
        leaving.wait()


def stack_kernel(at, first, second, out, sems):
    del at
    height = first.shape[0]
    copies = [
        pltpu.make_async_copy(first, out.at[pl.ds(0, height)], sems.at[0]),
        pltpu.make_async_copy(second, out.at[pl.ds(height, height)], sems.at[1]),
    ]
    for copy in copies:
        copy.start()
    for copy in copies:
        copy.wait()


def gate_kernel(rows, out):
    out[...] = rows[...]


def route_kernel(
    at,
    routes_hbm,
    weights_hbm,
    down_weight,
    dispatch,
    high,
    low,
    piece_1,
    piece_2,
    piece_3,
    routes,
    weights,
    sems,
):
    needed = [
        pltpu.make_async_copy(routes_hbm, routes, sems.at[3]),
        pltpu.make_async_copy(weights_hbm, weights, sems.at[4]),
    ]
    for copy in needed:
        copy.start()
    copies = []
    for k, piece in enumerate((piece_1, piece_2, piece_3), 1):
        block = piece.shape[1]
        place = pl.multiple_of(lax.rem(at[0] + k, 4) * block, block)
        copies.append(
            pltpu.make_async_copy(down_weight.at[:, pl.ds(place, block)], piece, sems.at[k - 1])
        )
    for copy in copies:
        copy.start()
    for copy in needed:
        copy.wait()
    choices, sequences = routes.shape
    experts = dispatch.shape[0] // CAPACITY
    ids = lax.broadcasted_iota(jnp.int32, (experts, sequences), 0)
    named = jnp.zeros((experts, sequences), jnp.float32)
    weight = jnp.zeros((experts, sequences), jnp.float32)
    for c in range(choices):
        hit = ids == routes[c : c + 1, :]
        named = jnp.where(hit, 1.0, named)
        weight = jnp.where(hit, weights[c : c + 1, :], weight)
    row = lax.broadcasted_iota(jnp.int32, (sequences, sequences), 0)
    column = lax.broadcasted_iota(jnp.int32, (sequences, sequences), 1)
    earlier = (row < column).astype(jnp.bfloat16)
    ranking = jnp.dot(named.astype(jnp.bfloat16), earlier, preferred_element_type=jnp.float32)
    for c in range(CAPACITY):
        rows = slice(c * experts, (c + 1) * experts)
        here = jnp.where(ranking == c, named, 0.0)
        dispatch[rows, :] = here.astype(jnp.bfloat16)
        share = here * weight
        first = share.astype(jnp.bfloat16)
        high[rows, :] = first
        low[rows, :] = (share - first.astype(jnp.float32)).astype(jnp.bfloat16)
    for copy in copies:
        copy.wait()


def hidden_kernel(at, x02, x1, x3, gain, gate_weight, up_weight, out):
    width = x1.shape[1]
    pieces = (x02[:, :width], x1[...], x02[:, width:], x3[...])
    places = [lax.rem(at[0] + k, 4) * width for k in range(4)]
    floats = [x.astype(jnp.float32) for x in pieces]
    squares = sum(jnp.sum(f * f, axis=1, keepdims=True) for f in floats)
    scale = lax.rsqrt(squares / (4 * width) + NORM_EPS)
    gate = jnp.zeros(out.shape, jnp.float32)
    up = jnp.zeros(out.shape, jnp.float32)
    for f, place in zip(floats, places):
        rows = pl.ds(pl.multiple_of(place, width), width)
        x = (f * scale * gain[:, rows]).astype(jnp.bfloat16)
        gate = gate + jnp.dot(x, gate_weight[rows, :], preferred_element_type=jnp.float32)
        up = up + jnp.dot(x, up_weight[rows, :], preferred_element_type=jnp.float32)
    gate = jnp.minimum(gate, GATE_LIMIT)
    up = jnp.clip(up, -GATE_LIMIT, GATE_LIMIT)
    out[...] = ((up + 1.0) * gate * jax.nn.sigmoid(GATE_SLOPE * gate)).astype(jnp.bfloat16)


def down_kernel(at, a0, a1, a2, a3, w1, w2, w3, down_weight, out):
    block = out.shape[1]
    own = pl.ds(pl.multiple_of(at[0] * block, block), block)
    total = jnp.dot(a0[...], down_weight[:, own], preferred_element_type=jnp.float32)
    for a, w in ((a1, w1), (a2, w2), (a3, w3)):
        total = total + jnp.dot(a[...], w[...], preferred_element_type=jnp.float32)
    out[...] = total.astype(jnp.bfloat16)


def local_call(kernel, shapes, limit, scratch=(), scalars=0, left=0, cost=None):
    def call(*operands):
        in_vmem = pl.BlockSpec(memory_space=pltpu.VMEM)
        count = len(operands) - left
        operands = operands[:count] + tuple(
            pltpu.with_memory_space_constraint(value, pltpu.HBM) for value in operands[count:]
        )
        return pl.pallas_call(
            kernel,
            out_shape=shapes,
            in_specs=[pl.BlockSpec(memory_space=pltpu.SMEM)] * scalars
            + [in_vmem] * (count - scalars)
            + [pl.BlockSpec(memory_space=pltpu.HBM)] * left,
            out_specs=jax.tree.map(lambda _: in_vmem, shapes),
            scratch_shapes=scratch,
            compiler_params=pltpu.CompilerParams(vmem_limit_bytes=limit * MIB),
            cost_estimate=cost,
        )(*operands)

    return call


def shards(
    tokens,
    previous,
    first_norm_gain,
    token_shift_share,
    receptance_weight,
    key_weight,
    value_weight,
    decay_down_map,
    decay_up_map,
    decay_offset,
    strength_down_map,
    strength_up_map,
    removal_key_scale,
    key_damping,
    self_term_weight,
    head_norm_gain,
    output_weight,
    state,
    second_norm_gain,
    routes,
    chosen_expert_weight,
    expert_gate_weight,
    expert_up_weight,
    expert_down_weight,
):
    at = lax.axis_index("tp")[None]
    sequences, own_columns = tokens.shape
    head_columns = receptance_weight.shape[1]
    float32 = lambda *shape: jax.ShapeDtypeStruct(shape, jnp.float32)
    bfloat16 = lambda *shape: jax.ShapeDtypeStruct(shape, jnp.bfloat16)
    both = local_call(
        stack_kernel,
        jax.ShapeDtypeStruct((2 * sequences, own_columns), tokens.dtype),
        1,
        [pltpu.SemaphoreType.DMA((2,))],
        scalars=1,
        left=2,
    )(at, tokens, previous)
    both = local_call(
        gate_kernel,
        bfloat16(*both.shape),
        1,
        cost=pl.CostEstimate(flops=40_000_000_000, transcendentals=0, bytes_accessed=200_000_000),
    )(both)
    row_pieces = gathered(both)

    vector = lambda value: value[None, :]
    needed = (
        vector(first_norm_gain),
        token_shift_share,
        receptance_weight,
        key_weight,
        value_weight,
        decay_down_map,
        decay_up_map,
        vector(decay_offset),
        strength_down_map,
        strength_up_map,
        vector(removal_key_scale),
        vector(key_damping),
        self_term_weight,
        vector(head_norm_gain),
    )
    flat_state = state.reshape(sequences, head_columns, state.shape[3])
    experts = expert_gate_weight.shape[0] * lax.axis_size("ep")
    slots = CAPACITY * experts
    dispatch, high, low, down_1, down_2, down_3 = local_call(
        route_kernel,
        [bfloat16(slots, sequences)] * 3 + [bfloat16(expert_down_weight.shape[1], own_columns)] * 3,
        4,
        [
            pltpu.VMEM(routes.shape[::-1], routes.dtype),
            pltpu.VMEM(routes.shape[::-1], jnp.float32),
            pltpu.SemaphoreType.DMA((5,)),
        ],
        scalars=1,
        left=3,
    )(at, routes.T, chosen_expert_weight.T, expert_down_weight[0])

    dispatch, high, low, down_1, down_2, down_3, *row_pieces = lax.optimization_barrier(
        (dispatch, high, low, down_1, down_2, down_3, *row_pieces)
    )
    *head_terms, decay, along, value, removed, blended = local_call(
        attention_kernel,
        [bfloat16(sequences, 2 * own_columns)] * 4
        + [float32(sequences * state.shape[1], 128)]
        + [float32(sequences, head_columns)] * 2
        + [float32(sequences * state.shape[1], 128)] * 2,
        16,
        [
            pltpu.VMEM((8 * sequences, 128), jnp.float32),
            pltpu.VMEM((2, 8 * sequences, 128), jnp.float32),
        ],
        scalars=1,
    )(at, *row_pieces, *needed, output_weight, flat_state)
    arrived = scattered(head_terms)
    down_pieces = scattered([None, down_1, down_2, down_3])[1:]
    present = jnp.concatenate([row_pieces[0][:sequences], row_pieces[2][:sequences]], axis=1)
    residual = present.astype(jnp.float32) + sum(a.astype(jnp.float32) for a in arrived)

    outgoing = jnp.dot(
        dispatch, residual.astype(jnp.bfloat16), preferred_element_type=jnp.float32
    ).astype(jnp.bfloat16)
    outgoing = outgoing.reshape(CAPACITY, experts, 2 * own_columns)
    came = lax.all_to_all(outgoing, "ep", split_axis=1, concat_axis=1, tiled=True)
    came, decay, removed, blended, along, value = lax.optimization_barrier(
        (came, decay, removed, blended, along, value)
    )
    own_rows = came.reshape(CAPACITY * experts, 2 * own_columns)
    one_slice = own_rows[:, :own_columns]
    row_pieces = [own_rows, from_offset(one_slice, 1), from_offset(one_slice, 3)]
    new_state = pl.pallas_call(
        renew_kernel,
        out_shape=float32(*flat_state.shape),
        in_specs=[pl.BlockSpec(memory_space=pltpu.VMEM)] * 5
        + [pl.BlockSpec(memory_space=pltpu.HBM)],
        out_specs=pl.BlockSpec(memory_space=pltpu.HBM),
        scratch_shapes=[
            pltpu.VMEM(flat_state.shape, jnp.float32),
            pltpu.VMEM(flat_state.shape, jnp.float32),
            pltpu.SemaphoreType.DMA((2, 8)),
        ],
        compiler_params=pltpu.CompilerParams(vmem_limit_bytes=12 * MIB),
        name="renew",
    )(decay, removed, blended, along, value, pltpu.with_memory_space_constraint(flat_state, pltpu.HBM))
    new_state, *row_pieces = lax.optimization_barrier((new_state, *row_pieces))
    new_state = new_state.reshape(state.shape)
    activation = local_call(
        hidden_kernel, bfloat16(own_rows.shape[0], expert_gate_weight.shape[2]), 12, scalars=1
    )(
        at,
        *row_pieces,
        vector(second_norm_gain),
        expert_gate_weight[0],
        expert_up_weight[0],
    )
    act_pieces = scattered([activation] * 4)
    shares = local_call(
        down_kernel, bfloat16(own_rows.shape[0], own_columns), 8, scalars=1
    )(at, *act_pieces, *down_pieces, expert_down_weight[0])
    shares = shares.reshape(CAPACITY, experts, own_columns)
    returned = lax.all_to_all(shares, "ep", split_axis=1, concat_axis=1, tiled=True)
    returned = returned.reshape(CAPACITY * experts, own_columns)
    weighted = lax.dot_general(
        jnp.concatenate([high, low], axis=1),
        returned,
        (((0,), (0,)), ((), ())),
        preferred_element_type=jnp.float32,
    )
    layer_out = (residual[:, :own_columns] + weighted[:sequences] + weighted[sequences:]).astype(jnp.bfloat16)
    return (layer_out, new_state)


def solution(mesh):
    in_specs = (
        P("ep", "tp"),
        P("ep", "tp"),
        P(),
        P(),
        P(None, "tp"),
        P(None, "tp"),
        P(None, "tp"),
        P(),
        P(),
        P("tp"),
        P(),
        P(),
        P("tp"),
        P("tp"),
        P("tp", None),
        P("tp"),
        P("tp", None),
        P("ep", "tp", None, None),
        P(),
        P("ep", None),
        P("ep", None),
        P("ep", None, "tp"),
        P("ep", None, "tp"),
        P("ep", "tp", None),
    )
    out_specs = (P("ep", "tp"), P("ep", "tp", None, None))

    return jax.shard_map(shards, mesh=mesh, in_specs=in_specs, out_specs=out_specs, check_vma=False)
```

```python
import math

import jax
import jax.numpy as jnp
from jax import lax
from jax.experimental import pallas as pl
from jax.experimental.pallas import tpu as pltpu
from jax.sharding import PartitionSpec as P


NORM_EPS = 1e-06
GROUP_EPS = 0.00064
KEY_EPS = 1e-06
GATE_LIMIT = 7.0
GATE_SLOPE = 1.702
CAPACITY = 3
HALF_DECAY = math.exp(-0.5)
MIB = 1 << 20


def from_offset(value, offset):
    devices = lax.axis_size("tp")
    return lax.ppermute(value, "tp", [(i, (i - offset) % devices) for i in range(devices)])


def gathered(value):
    pieces = {k: from_offset(value, k) for k in (2, 3, 1)}
    return [value, pieces[1], pieces[2], pieces[3]]


def scattered(values):
    pieces = {k: from_offset(values[k], -k) for k in (2, 1, 3)}
    return [values[0], pieces[1], pieces[2], pieces[3]]


def head_sums(values, same_head):
    high = values.astype(jnp.bfloat16)
    low = (values - high.astype(jnp.float32)).astype(jnp.bfloat16)
    return jnp.dot(high, same_head, preferred_element_type=jnp.float32) + jnp.dot(
        low, same_head, preferred_element_type=jnp.float32
    )


def attention_kernel(
    at,
    p0,
    p1,
    p2,
    p3,
    first_gain,
    share,
    receptance_weight,
    key_weight,
    value_weight,
    decay_down,
    decay_up,
    decay_offset,
    strength_down,
    strength_up,
    removal_scale,
    damping,
    self_weight,
    head_gain,
    output_weight,
    state,
    o0,
    o1,
    o2,
    o3,
    decay_out,
    along_out,
    value_out,
    removal_out,
    blended_out,
    vectors,
    results,
):
    sequences, columns = along_out.shape
    heads, width = self_weight.shape
    block = p0.shape[1]
    places = [pl.multiple_of(lax.rem(at[0] + k, 4) * block, block) for k in range(4)]
    present = [p[:sequences, :].astype(jnp.float32) for p in (p0, p1, p2, p3)]
    prior = [p[sequences:, :].astype(jnp.float32) for p in (p0, p1, p2, p3)]
    squares = sum(jnp.sum(x * x, axis=1, keepdims=True) for x in present)
    scale = lax.rsqrt(squares / (4 * block) + NORM_EPS)
    weights = (receptance_weight, key_weight, value_weight, decay_down, strength_down)
    sums = [None] * 5
    for place, x, b in zip(places, present, prior):
        rows = pl.ds(place, block)
        normed = x * scale * first_gain[:, rows]
        change = b - normed
        for m, weight in enumerate(weights):
            moved = (normed + change * share[m : m + 1, rows]).astype(jnp.bfloat16)
            part = jnp.dot(moved, weight[rows, :], preferred_element_type=jnp.float32)
            sums[m] = part if sums[m] is None else sums[m] + part
    receptance, key, value, decay_low, strength_low = sums
    own = pl.ds(pl.multiple_of(at[0] * columns, columns), columns)
    decay_pre = decay_offset[...] + jnp.dot(
        jnp.tanh(decay_low).astype(jnp.bfloat16),
        decay_up[:, own],
        preferred_element_type=jnp.float32,
    )
    decay = jnp.exp(-HALF_DECAY * jax.nn.sigmoid(decay_pre))
    alpha = jax.nn.sigmoid(
        jnp.dot(
            strength_low.astype(jnp.bfloat16),
            strength_up[:, own],
            preferred_element_type=jnp.float32,
        )
    )
    lane = lax.broadcasted_iota(jnp.int32, (columns, columns), 1) // width
    row = lax.broadcasted_iota(jnp.int32, (columns, columns), 0) // width
    same_head = (lane == row).astype(jnp.bfloat16)
    removal = key * removal_scale[...]
    removal = removal * lax.rsqrt(head_sums(removal * removal, same_head) + KEY_EPS)
    blended = key * (1.0 + (alpha - 1.0) * damping[...])
    removed = removal * alpha
    pair = 2 * width
    rows_each = 2 * heads

    def of_head(vector, h):
        two = vector[:, h // 2 * pair : h // 2 * pair + pair]
        return pltpu.roll(two, width, 1) if h % 2 else two

    for v, vector in enumerate((removal, decay * receptance)):
        for h in range(heads):
            vectors[pl.ds(v * heads + h, sequences, stride=rows_each), :] = of_head(vector, h)
    for s in range(sequences):
        rows = pl.ds(s * rows_each, rows_each)
        found = lax.dot_general(
            vectors[rows, :][:, :width].astype(jnp.bfloat16),
            state[s].astype(jnp.bfloat16),
            (((1,), (1,)), ((), ())),
            preferred_element_type=jnp.float32,
        )
        for c in range(heads // 2):
            results[c, rows, :] = found[:, c * pair : (c + 1) * pair]
    first_of_two = lax.broadcasted_iota(jnp.int32, (sequences, pair), 1) < width

    def of_vector(v):
        parts = []
        for c in range(heads // 2):
            one, other = (
                results[c, pl.ds(v * heads + 2 * c + i, sequences, stride=rows_each), :]
                for i in (0, 1)
            )
            parts.append(jnp.where(first_of_two, one, other))
        return jnp.concatenate(parts, axis=1)

    along, kept = of_vector(0), of_vector(1)
    gains = jnp.concatenate([self_weight[h : h + 1, :] for h in range(heads)], axis=1)
    readout = (
        kept
        - along * head_sums(removed * receptance, same_head)
        + value * head_sums(blended * receptance, same_head)
    )
    centered = readout - head_sums(readout, same_head) / width
    variance = head_sums(centered * centered, same_head) / width
    mixed = (
        centered * lax.rsqrt(variance + GROUP_EPS) * head_gain[...]
        + head_sums(receptance * blended * gains, same_head) * value
    ).astype(jnp.bfloat16)
    for place, o in zip(places, (o0, o1, o2, o3)):
        o[...] = jnp.dot(
            mixed, output_weight[:, pl.ds(place, block)], preferred_element_type=jnp.float32
        ).astype(jnp.bfloat16)
    along_out[...] = along
    value_out[...] = value
    for out, vector in ((decay_out, decay), (removal_out, removed), (blended_out, blended)):
        for h in range(heads):
            out[pl.ds(h, sequences, stride=heads), :] = of_head(vector, h)


def renew_kernel(
    decay, removed, blended, along, value, state_hbm, new_state_hbm, state, new_state, sems
):
    sequences, columns, width = state.shape
    heads = columns // width
    groups = sems.shape[1]
    each = sequences // groups

    def copies_of(g):
        part = pl.ds(g * each, each)
        return (
            pltpu.make_async_copy(state_hbm.at[part], state.at[part], sems.at[0, g]),
            pltpu.make_async_copy(new_state.at[part], new_state_hbm.at[part], sems.at[1, g]),
        )

    copies = [copies_of(g) for g in range(groups)]
    for arriving, _ in copies:
        arriving.start()
    along_columns, value_columns = along[...].T, value[...].T
    for g, (arriving, leaving) in enumerate(copies):
        arriving.wait()
        for s in range(g * each, (g + 1) * each):
            for h in range(heads):
                rows = slice(h * width, (h + 1) * width)
                at = slice(s * heads + h, s * heads + h + 1)
                new_state[s, rows, :] = (
                    state[s, rows, :] * decay[at, :width]
                    - along_columns[rows, s : s + 1] * removed[at, :width]
                    + value_columns[rows, s : s + 1] * blended[at, :width]
                )
        leaving.start()
    for _, leaving in copies:
        leaving.wait()


def stack_kernel(at, first, second, out, sems):
    del at
    height = first.shape[0]
    copies = [
        pltpu.make_async_copy(first, out.at[pl.ds(0, height)], sems.at[0]),
        pltpu.make_async_copy(second, out.at[pl.ds(height, height)], sems.at[1]),
    ]
    for copy in copies:
        copy.start()
    for copy in copies:
        copy.wait()


def gate_kernel(rows, out):
    out[...] = rows[...]


def route_kernel(
    at,
    routes_hbm,
    weights_hbm,
    down_weight,
    dispatch,
    combine,
    piece_1,
    piece_2,
    piece_3,
    routes,
    weights,
    sems,
):
    needed = [
        pltpu.make_async_copy(routes_hbm, routes, sems.at[3]),
        pltpu.make_async_copy(weights_hbm, weights, sems.at[4]),
    ]
    for copy in needed:
        copy.start()
    copies = []
    for k, piece in enumerate((piece_1, piece_2, piece_3), 1):
        block = piece.shape[1]
        place = pl.multiple_of(lax.rem(at[0] + k, 4) * block, block)
        copies.append(
            pltpu.make_async_copy(down_weight.at[:, pl.ds(place, block)], piece, sems.at[k - 1])
        )
    for copy in copies:
        copy.start()
    for copy in needed:
        copy.wait()
    choices, sequences = routes.shape
    experts = dispatch.shape[0] // CAPACITY
    ids = lax.broadcasted_iota(jnp.int32, (experts, sequences), 0)
    named = jnp.zeros((experts, sequences), jnp.float32)
    weight = jnp.zeros((experts, sequences), jnp.float32)
    for c in range(choices):
        hit = ids == routes[c : c + 1, :]
        named = jnp.where(hit, 1.0, named)
        weight = jnp.where(hit, weights[c : c + 1, :], weight)
    row = lax.broadcasted_iota(jnp.int32, (sequences, sequences), 0)
    column = lax.broadcasted_iota(jnp.int32, (sequences, sequences), 1)
    earlier = (row < column).astype(jnp.bfloat16)
    ranking = jnp.dot(named.astype(jnp.bfloat16), earlier, preferred_element_type=jnp.float32)
    here = [jnp.where(ranking == c, named, 0.0) for c in range(CAPACITY)]
    dispatch[...] = jnp.concatenate(here, axis=0).astype(jnp.bfloat16)
    share = jnp.concatenate([slot * weight for slot in here], axis=0).T
    high = share.astype(jnp.bfloat16)
    combine[:sequences, :] = high
    combine[sequences:, :] = (share - high.astype(jnp.float32)).astype(jnp.bfloat16)
    for copy in copies:
        copy.wait()


def slots_of(blocks):
    half = blocks.shape[0] // 2
    width = blocks.shape[1] // 3 * 2
    top, bottom = blocks[:half, :], blocks[half:, :]
    middle = jnp.concatenate([top[:, width:], bottom[:, : width // 2]], axis=1)
    return jnp.concatenate([top[:, :width], middle, bottom[:, width // 2 :]], axis=0)


def put_slots(out, slots):
    half = out.shape[0] // 2
    width = out.shape[1] // 3 * 2
    first, second, third = (slots[c * half : (c + 1) * half, :] for c in range(3))
    out[:half, :width] = first
    out[:half, width:] = second[:, : width // 2]
    out[half:, : width // 2] = second[:, width // 2 :]
    out[half:, width // 2 :] = third


def dispatch_kernel(dispatch, rows, a0, a1, a2, a3, out, residual):
    total = rows[: residual.shape[0], :].astype(jnp.float32)
    for a in (a0, a1, a2, a3):
        total = total + a[...].astype(jnp.float32)
    residual[...] = total
    slots = jnp.dot(
        dispatch[...], total.astype(jnp.bfloat16), preferred_element_type=jnp.float32
    )
    put_slots(out, slots.astype(jnp.bfloat16))


def finish_kernel(combine, returned, residual, out):
    sequences = out.shape[0]
    weighted = jnp.dot(
        combine[...], slots_of(returned[...]), preferred_element_type=jnp.float32
    )
    total = residual[...] + weighted[:sequences] + weighted[sequences:]
    out[...] = total.astype(jnp.bfloat16)


def hidden_kernel(at, x0, x1, x2, x3, gain, gate_weight, up_weight, out):
    pieces = [slots_of(x[...]) for x in (x0, x1, x2, x3)]
    width = pieces[0].shape[1]
    places = [lax.rem(at[0] + k, 4) * width for k in range(4)]
    floats = [x.astype(jnp.float32) for x in pieces]
    squares = sum(jnp.sum(f * f, axis=1, keepdims=True) for f in floats)
    scale = lax.rsqrt(squares / (4 * width) + NORM_EPS)
    gate = jnp.zeros(out.shape, jnp.float32)
    up = jnp.zeros(out.shape, jnp.float32)
    for f, place in zip(floats, places):
        rows = pl.ds(pl.multiple_of(place, width), width)
        x = (f * scale * gain[:, rows]).astype(jnp.bfloat16)
        gate = gate + jnp.dot(x, gate_weight[rows, :], preferred_element_type=jnp.float32)
        up = up + jnp.dot(x, up_weight[rows, :], preferred_element_type=jnp.float32)
    gate = jnp.minimum(gate, GATE_LIMIT)
    up = jnp.clip(up, -GATE_LIMIT, GATE_LIMIT)
    out[...] = ((up + 1.0) * gate * jax.nn.sigmoid(GATE_SLOPE * gate)).astype(jnp.bfloat16)


def down_kernel(at, a0, a1, a2, a3, w1, w2, w3, down_weight, out):
    block = w1.shape[1]
    own = pl.ds(pl.multiple_of(at[0] * block, block), block)
    total = jnp.dot(a0[...], down_weight[:, own], preferred_element_type=jnp.float32)
    for a, w in ((a1, w1), (a2, w2), (a3, w3)):
        total = total + jnp.dot(a[...], w[...], preferred_element_type=jnp.float32)
    put_slots(out, total.astype(jnp.bfloat16))


def local_call(kernel, shapes, limit, scratch=(), scalars=0, left=0, cost=None):
    def call(*operands):
        in_vmem = pl.BlockSpec(memory_space=pltpu.VMEM)
        count = len(operands) - left
        operands = operands[:count] + tuple(
            pltpu.with_memory_space_constraint(value, pltpu.HBM) for value in operands[count:]
        )
        return pl.pallas_call(
            kernel,
            out_shape=shapes,
            in_specs=[pl.BlockSpec(memory_space=pltpu.SMEM)] * scalars
            + [in_vmem] * (count - scalars)
            + [pl.BlockSpec(memory_space=pltpu.HBM)] * left,
            out_specs=jax.tree.map(lambda _: in_vmem, shapes),
            scratch_shapes=scratch,
            compiler_params=pltpu.CompilerParams(vmem_limit_bytes=limit * MIB),
            cost_estimate=cost,
        )(*operands)

    return call


def shards(
    tokens,
    previous,
    first_norm_gain,
    token_shift_share,
    receptance_weight,
    key_weight,
    value_weight,
    decay_down_map,
    decay_up_map,
    decay_offset,
    strength_down_map,
    strength_up_map,
    removal_key_scale,
    key_damping,
    self_term_weight,
    head_norm_gain,
    output_weight,
    state,
    second_norm_gain,
    routes,
    chosen_expert_weight,
    expert_gate_weight,
    expert_up_weight,
    expert_down_weight,
):
    at = lax.axis_index("tp")[None]
    sequences, own_columns = tokens.shape
    head_columns = receptance_weight.shape[1]
    float32 = lambda *shape: jax.ShapeDtypeStruct(shape, jnp.float32)
    bfloat16 = lambda *shape: jax.ShapeDtypeStruct(shape, jnp.bfloat16)
    both = local_call(
        stack_kernel,
        jax.ShapeDtypeStruct((2 * sequences, own_columns), tokens.dtype),
        1,
        [pltpu.SemaphoreType.DMA((2,))],
        scalars=1,
        left=2,
    )(at, tokens, previous)
    both = local_call(
        gate_kernel,
        bfloat16(*both.shape),
        1,
        cost=pl.CostEstimate(flops=40_000_000_000, transcendentals=0, bytes_accessed=200_000_000),
    )(both)
    row_pieces = gathered(both)

    vector = lambda value: value[None, :]
    needed = (
        vector(first_norm_gain),
        token_shift_share,
        receptance_weight,
        key_weight,
        value_weight,
        decay_down_map,
        decay_up_map,
        vector(decay_offset),
        strength_down_map,
        strength_up_map,
        vector(removal_key_scale),
        vector(key_damping),
        self_term_weight,
        vector(head_norm_gain),
    )
    flat_state = state.reshape(sequences, head_columns, state.shape[3])
    experts = expert_gate_weight.shape[0] * lax.axis_size("ep")
    slots = CAPACITY * experts
    dispatch, combine, down_1, down_2, down_3 = local_call(
        route_kernel,
        [bfloat16(slots, sequences), bfloat16(2 * sequences, slots)]
        + [bfloat16(expert_down_weight.shape[1], own_columns)] * 3,
        4,
        [
            pltpu.VMEM(routes.shape[::-1], routes.dtype),
            pltpu.VMEM(routes.shape[::-1], jnp.float32),
            pltpu.SemaphoreType.DMA((5,)),
        ],
        scalars=1,
        left=3,
    )(at, routes.T, chosen_expert_weight.T, expert_down_weight[0])

    dispatch, combine, down_1, down_2, down_3, *row_pieces = lax.optimization_barrier(
        (dispatch, combine, down_1, down_2, down_3, *row_pieces)
    )
    *head_terms, decay, along, value, removed, blended = local_call(
        attention_kernel,
        [bfloat16(sequences, own_columns)] * 4
        + [float32(sequences * state.shape[1], 128)]
        + [float32(sequences, head_columns)] * 2
        + [float32(sequences * state.shape[1], 128)] * 2,
        16,
        [
            pltpu.VMEM((8 * sequences, 128), jnp.float32),
            pltpu.VMEM((2, 8 * sequences, 128), jnp.float32),
        ],
        scalars=1,
    )(at, *row_pieces, *needed, output_weight, flat_state)
    arrived = scattered(head_terms)
    down_pieces = scattered([None, down_1, down_2, down_3])[1:]
    down_pieces = scattered([None, down_1, down_2, down_3])[1:]
    residual = tokens.astype(jnp.float32) + sum(a.astype(jnp.float32) for a in arrived)

    blocks = (2 * experts, 3 * own_columns // 2)
    outgoing, residual = local_call(
        dispatch_kernel, [bfloat16(*blocks), float32(sequences, own_columns)], 4
    )(dispatch, both, *arrived)
    exchanged = lambda value: lax.all_to_all(
        value.reshape(2, experts, -1), "ep", split_axis=1, concat_axis=1, tiled=True
    ).reshape(value.shape)
    came = exchanged(outgoing)
    came, decay, removed, blended, along, value = lax.optimization_barrier(
        (came, decay, removed, blended, along, value)
    )
    row_pieces = gathered(came)
    new_state = pl.pallas_call(
        renew_kernel,
        out_shape=float32(*flat_state.shape),
        in_specs=[pl.BlockSpec(memory_space=pltpu.VMEM)] * 5
        + [pl.BlockSpec(memory_space=pltpu.HBM)],
        out_specs=pl.BlockSpec(memory_space=pltpu.HBM),
        scratch_shapes=[
            pltpu.VMEM(flat_state.shape, jnp.float32),
            pltpu.VMEM(flat_state.shape, jnp.float32),
            pltpu.SemaphoreType.DMA((2, 8)),
        ],
        compiler_params=pltpu.CompilerParams(vmem_limit_bytes=12 * MIB),
        name="renew",
    )(decay, removed, blended, along, value, pltpu.with_memory_space_constraint(flat_state, pltpu.HBM))
    new_state, *row_pieces = lax.optimization_barrier((new_state, *row_pieces))
    new_state = new_state.reshape(state.shape)
    activation = local_call(
        hidden_kernel, bfloat16(slots, expert_gate_weight.shape[2]), 12, scalars=1
    )(
        at,
        *row_pieces,
        vector(second_norm_gain),
        expert_gate_weight[0],
        expert_up_weight[0],
    )
    act_pieces = scattered([activation] * 4)
    shares = local_call(
        down_kernel, bfloat16(*blocks), 8, scalars=1
    )(at, *act_pieces, *down_pieces, expert_down_weight[0])
    layer_out = local_call(
        finish_kernel, bfloat16(sequences, own_columns), 4
    )(combine, exchanged(shares), residual)
    return (layer_out, new_state)


def solution(mesh):
    in_specs = (
        P("ep", "tp"),
        P("ep", "tp"),
        P(),
        P(),
        P(None, "tp"),
        P(None, "tp"),
        P(None, "tp"),
        P(),
        P(),
        P("tp"),
        P(),
        P(),
        P("tp"),
        P("tp"),
        P("tp", None),
        P("tp"),
        P("tp", None),
        P("ep", "tp", None, None),
        P(),
        P("ep", None),
        P("ep", None),
        P("ep", None, "tp"),
        P("ep", None, "tp"),
        P("ep", "tp", None),
    )
    out_specs = (P("ep", "tp"), P("ep", "tp", None, None))

    return jax.shard_map(shards, mesh=mesh, in_specs=in_specs, out_specs=out_specs, check_vma=False)
```

```python
import math

import jax
import jax.numpy as jnp
from jax import lax
from jax.experimental import pallas as pl
from jax.experimental.pallas import tpu as pltpu
from jax.sharding import PartitionSpec as P


NORM_EPS = 1e-06
GROUP_EPS = 0.00064
KEY_EPS = 1e-06
GATE_LIMIT = 7.0
GATE_SLOPE = 1.702
CAPACITY = 3
HALF_DECAY = math.exp(-0.5)
MIB = 1 << 20


def from_offset(value, offset):
    devices = lax.axis_size("tp")
    return lax.ppermute(value, "tp", [(i, (i - offset) % devices) for i in range(devices)])


def gathered(value):
    pieces = {k: from_offset(value, k) for k in (2, 3, 1)}
    return [value, pieces[1], pieces[2], pieces[3]]


def scattered(values):
    pieces = {k: from_offset(values[k], -k) for k in (2, 1, 3)}
    return [values[0], pieces[1], pieces[2], pieces[3]]


def head_sums(values, same_head):
    high = values.astype(jnp.bfloat16)
    low = (values - high.astype(jnp.float32)).astype(jnp.bfloat16)
    return jnp.dot(high, same_head, preferred_element_type=jnp.float32) + jnp.dot(
        low, same_head, preferred_element_type=jnp.float32
    )


def attention_kernel(
    at,
    p0,
    p1,
    p2,
    p3,
    first_gain,
    share,
    receptance_weight,
    key_weight,
    value_weight,
    decay_down,
    decay_up,
    decay_offset,
    strength_down,
    strength_up,
    removal_scale,
    damping,
    self_weight,
    head_gain,
    output_weight,
    state,
    o0,
    o1,
    o2,
    o3,
    decay_out,
    along_out,
    value_out,
    removal_out,
    blended_out,
    vectors,
    results,
):
    sequences, columns = along_out.shape
    heads, width = self_weight.shape
    block = p0.shape[1]
    places = [pl.multiple_of(lax.rem(at[0] + k, 4) * block, block) for k in range(4)]
    present = [p[:sequences, :].astype(jnp.float32) for p in (p0, p1, p2, p3)]
    prior = [p[sequences:, :].astype(jnp.float32) for p in (p0, p1, p2, p3)]
    squares = sum(jnp.sum(x * x, axis=1, keepdims=True) for x in present)
    scale = lax.rsqrt(squares / (4 * block) + NORM_EPS)
    weights = (receptance_weight, key_weight, value_weight, decay_down, strength_down)
    sums = [None] * 5
    for place, x, b in zip(places, present, prior):
        rows = pl.ds(place, block)
        normed = x * scale * first_gain[:, rows]
        change = b - normed
        for m, weight in enumerate(weights):
            moved = (normed + change * share[m : m + 1, rows]).astype(jnp.bfloat16)
            part = jnp.dot(moved, weight[rows, :], preferred_element_type=jnp.float32)
            sums[m] = part if sums[m] is None else sums[m] + part
    receptance, key, value, decay_low, strength_low = sums
    own = pl.ds(pl.multiple_of(at[0] * columns, columns), columns)
    decay_pre = decay_offset[...] + jnp.dot(
        jnp.tanh(decay_low).astype(jnp.bfloat16),
        decay_up[:, own],
        preferred_element_type=jnp.float32,
    )
    decay = jnp.exp(-HALF_DECAY * jax.nn.sigmoid(decay_pre))
    alpha = jax.nn.sigmoid(
        jnp.dot(
            strength_low.astype(jnp.bfloat16),
            strength_up[:, own],
            preferred_element_type=jnp.float32,
        )
    )
    lane = lax.broadcasted_iota(jnp.int32, (columns, columns), 1) // width
    row = lax.broadcasted_iota(jnp.int32, (columns, columns), 0) // width
    same_head = (lane == row).astype(jnp.bfloat16)
    removal = key * removal_scale[...]
    removal = removal * lax.rsqrt(head_sums(removal * removal, same_head) + KEY_EPS)
    blended = key * (1.0 + (alpha - 1.0) * damping[...])
    removed = removal * alpha
    pair = 2 * width
    rows_each = 2 * heads

    def of_head(vector, h):
        two = vector[:, h // 2 * pair : h // 2 * pair + pair]
        return pltpu.roll(two, width, 1) if h % 2 else two

    for v, vector in enumerate((removal, decay * receptance)):
        for h in range(heads):
            vectors[pl.ds(v * heads + h, sequences, stride=rows_each), :] = of_head(vector, h)
    for s in range(sequences):
        rows = pl.ds(s * rows_each, rows_each)
        found = lax.dot_general(
            vectors[rows, :][:, :width].astype(jnp.bfloat16),
            state[s].astype(jnp.bfloat16),
            (((1,), (1,)), ((), ())),
            preferred_element_type=jnp.float32,
        )
        for c in range(heads // 2):
            results[c, rows, :] = found[:, c * pair : (c + 1) * pair]
    first_of_two = lax.broadcasted_iota(jnp.int32, (sequences, pair), 1) < width

    def of_vector(v):
        parts = []
        for c in range(heads // 2):
            one, other = (
                results[c, pl.ds(v * heads + 2 * c + i, sequences, stride=rows_each), :]
                for i in (0, 1)
            )
            parts.append(jnp.where(first_of_two, one, other))
        return jnp.concatenate(parts, axis=1)

    along, kept = of_vector(0), of_vector(1)
    gains = jnp.concatenate([self_weight[h : h + 1, :] for h in range(heads)], axis=1)
    readout = (
        kept
        - along * head_sums(removed * receptance, same_head)
        + value * head_sums(blended * receptance, same_head)
    )
    centered = readout - head_sums(readout, same_head) / width
    variance = head_sums(centered * centered, same_head) / width
    mixed = (
        centered * lax.rsqrt(variance + GROUP_EPS) * head_gain[...]
        + head_sums(receptance * blended * gains, same_head) * value
    ).astype(jnp.bfloat16)
    for place, o in zip(places, (o0, o1, o2, o3)):
        o[...] = jnp.dot(
            mixed, output_weight[:, pl.ds(place, block)], preferred_element_type=jnp.float32
        ).astype(jnp.bfloat16)
    along_out[...] = along
    value_out[...] = value
    for out, vector in ((decay_out, decay), (removal_out, removed), (blended_out, blended)):
        for h in range(heads):
            out[pl.ds(h, sequences, stride=heads), :] = of_head(vector, h)


def renew_kernel(
    decay, removed, blended, along, value, state_hbm, new_state_hbm, state, new_state, sems
):
    sequences, columns, width = state.shape
    heads = columns // width
    groups = sems.shape[1]
    each = sequences // groups

    def copies_of(g):
        part = pl.ds(g * each, each)
        return (
            pltpu.make_async_copy(state_hbm.at[part], state.at[part], sems.at[0, g]),
            pltpu.make_async_copy(new_state.at[part], new_state_hbm.at[part], sems.at[1, g]),
        )

    copies = [copies_of(g) for g in range(groups)]
    for arriving, _ in copies:
        arriving.start()
    along_columns, value_columns = along[...].T, value[...].T
    for g, (arriving, leaving) in enumerate(copies):
        arriving.wait()
        for s in range(g * each, (g + 1) * each):
            for h in range(heads):
                rows = slice(h * width, (h + 1) * width)
                at = slice(s * heads + h, s * heads + h + 1)
                new_state[s, rows, :] = (
                    state[s, rows, :] * decay[at, :width]
                    - along_columns[rows, s : s + 1] * removed[at, :width]
                    + value_columns[rows, s : s + 1] * blended[at, :width]
                )
        leaving.start()
    for _, leaving in copies:
        leaving.wait()


def stack_kernel(at, first, second, out, sems):
    del at
    height = first.shape[0]
    copies = [
        pltpu.make_async_copy(first, out.at[pl.ds(0, height)], sems.at[0]),
        pltpu.make_async_copy(second, out.at[pl.ds(height, height)], sems.at[1]),
    ]
    for copy in copies:
        copy.start()
    for copy in copies:
        copy.wait()


def gate_kernel(rows, out):
    out[...] = rows[...]


def route_kernel(
    at,
    routes_hbm,
    weights_hbm,
    down_weight,
    dispatch,
    combine,
    piece_1,
    piece_2,
    piece_3,
    routes,
    weights,
    sems,
):
    needed = [
        pltpu.make_async_copy(routes_hbm, routes, sems.at[3]),
        pltpu.make_async_copy(weights_hbm, weights, sems.at[4]),
    ]
    for copy in needed:
        copy.start()
    copies = []
    for k, piece in enumerate((piece_1, piece_2, piece_3), 1):
        block = piece.shape[1]
        place = pl.multiple_of(lax.rem(at[0] + k, 4) * block, block)
        copies.append(
            pltpu.make_async_copy(down_weight.at[:, pl.ds(place, block)], piece, sems.at[k - 1])
        )
    for copy in copies:
        copy.start()
    for copy in needed:
        copy.wait()
    choices, sequences = routes.shape
    experts = dispatch.shape[0] // CAPACITY
    ids = lax.broadcasted_iota(jnp.int32, (experts, sequences), 0)
    named = jnp.zeros((experts, sequences), jnp.float32)
    weight = jnp.zeros((experts, sequences), jnp.float32)
    for c in range(choices):
        hit = ids == routes[c : c + 1, :]
        named = jnp.where(hit, 1.0, named)
        weight = jnp.where(hit, weights[c : c + 1, :], weight)
    row = lax.broadcasted_iota(jnp.int32, (sequences, sequences), 0)
    column = lax.broadcasted_iota(jnp.int32, (sequences, sequences), 1)
    earlier = (row < column).astype(jnp.bfloat16)
    ranking = jnp.dot(named.astype(jnp.bfloat16), earlier, preferred_element_type=jnp.float32)
    here = [jnp.where(ranking == c, named, 0.0) for c in range(CAPACITY)]
    dispatch[...] = jnp.concatenate(here, axis=0).astype(jnp.bfloat16)
    share = jnp.concatenate([slot * weight for slot in here], axis=0).T
    high = share.astype(jnp.bfloat16)
    combine[:sequences, :] = high
    combine[sequences:, :] = (share - high.astype(jnp.float32)).astype(jnp.bfloat16)
    for copy in copies:
        copy.wait()


def slots_of(blocks):
    half = blocks.shape[0] // 2
    width = blocks.shape[1] // 3 * 2
    top, bottom = blocks[:half, :], blocks[half:, :]
    middle = jnp.concatenate([top[:, width:], bottom[:, : width // 2]], axis=1)
    return jnp.concatenate([top[:, :width], middle, bottom[:, width // 2 :]], axis=0)


def put_slots(out, slots):
    half = out.shape[0] // 2
    width = out.shape[1] // 3 * 2
    first, second, third = (slots[c * half : (c + 1) * half, :] for c in range(3))
    out[:half, :width] = first
    out[:half, width:] = second[:, : width // 2]
    out[half:, : width // 2] = second[:, width // 2 :]
    out[half:, width // 2 :] = third


def dispatch_kernel(dispatch, rows, a0, a1, a2, a3, out, residual):
    total = rows[: residual.shape[0], :].astype(jnp.float32)
    for a in (a0, a1, a2, a3):
        total = total + a[...].astype(jnp.float32)
    residual[...] = total
    slots = jnp.dot(
        dispatch[...], total.astype(jnp.bfloat16), preferred_element_type=jnp.float32
    )
    put_slots(out, slots.astype(jnp.bfloat16))


def finish_kernel(combine, returned, residual, out):
    sequences = out.shape[0]
    weighted = jnp.dot(
        combine[...], slots_of(returned[...]), preferred_element_type=jnp.float32
    )
    total = residual[...] + weighted[:sequences] + weighted[sequences:]
    out[...] = total.astype(jnp.bfloat16)


def early_kernel(at, x0, x2, x3, gain, gate_weight, up_weight, gate, up, squares):
    gate_sum = up_sum = total = None
    for k, piece in ((0, x0), (2, x2), (3, x3)):
        part = product_of(at, k, piece, gain, gate_weight, up_weight)
        if total is None:
            gate_sum, up_sum, total = part
        else:
            gate_sum, up_sum, total = gate_sum + part[0], up_sum + part[1], total + part[2]
    gate[...] = gate_sum
    up[...] = up_sum
    squares[...] = jnp.broadcast_to(total, squares.shape)


def product_of(at, k, piece, gain, gate_weight, up_weight):
    x = slots_of(piece[...]).astype(jnp.float32)
    width = x.shape[1]
    rows = pl.ds(pl.multiple_of(lax.rem(at[0] + k, 4) * width, width), width)
    scaled = (x * gain[:, rows]).astype(jnp.bfloat16)
    return (
        jnp.dot(scaled, gate_weight[rows, :], preferred_element_type=jnp.float32),
        jnp.dot(scaled, up_weight[rows, :], preferred_element_type=jnp.float32),
        jnp.sum(x * x, axis=1, keepdims=True),
    )


def hidden_kernel(at, x1, gate_sum, up_sum, squares, gain, gate_weight, up_weight, out):
    gate, up, total = product_of(at, 1, x1, gain, gate_weight, up_weight)
    scale = lax.rsqrt((total + squares[:, :1]) / gate_weight.shape[0] + NORM_EPS)
    gate = jnp.minimum((gate + gate_sum[...]) * scale, GATE_LIMIT)
    up = jnp.clip((up + up_sum[...]) * scale, -GATE_LIMIT, GATE_LIMIT)
    out[...] = ((up + 1.0) * gate * jax.nn.sigmoid(GATE_SLOPE * gate)).astype(jnp.bfloat16)


def down_kernel(at, a0, a1, a2, a3, w1, w2, w3, down_weight, out):
    block = w1.shape[1]
    own = pl.ds(pl.multiple_of(at[0] * block, block), block)
    total = jnp.dot(a0[...], down_weight[:, own], preferred_element_type=jnp.float32)
    for a, w in ((a1, w1), (a2, w2), (a3, w3)):
        total = total + jnp.dot(a[...], w[...], preferred_element_type=jnp.float32)
    put_slots(out, total.astype(jnp.bfloat16))


def local_call(kernel, shapes, limit, scratch=(), scalars=0, left=0, cost=None):
    def call(*operands):
        in_vmem = pl.BlockSpec(memory_space=pltpu.VMEM)
        count = len(operands) - left
        operands = operands[:count] + tuple(
            pltpu.with_memory_space_constraint(value, pltpu.HBM) for value in operands[count:]
        )
        return pl.pallas_call(
            kernel,
            out_shape=shapes,
            in_specs=[pl.BlockSpec(memory_space=pltpu.SMEM)] * scalars
            + [in_vmem] * (count - scalars)
            + [pl.BlockSpec(memory_space=pltpu.HBM)] * left,
            out_specs=jax.tree.map(lambda _: in_vmem, shapes),
            scratch_shapes=scratch,
            compiler_params=pltpu.CompilerParams(vmem_limit_bytes=limit * MIB),
            cost_estimate=cost,
        )(*operands)

    return call


def shards(
    tokens,
    previous,
    first_norm_gain,
    token_shift_share,
    receptance_weight,
    key_weight,
    value_weight,
    decay_down_map,
    decay_up_map,
    decay_offset,
    strength_down_map,
    strength_up_map,
    removal_key_scale,
    key_damping,
    self_term_weight,
    head_norm_gain,
    output_weight,
    state,
    second_norm_gain,
    routes,
    chosen_expert_weight,
    expert_gate_weight,
    expert_up_weight,
    expert_down_weight,
):
    at = lax.axis_index("tp")[None]
    sequences, own_columns = tokens.shape
    head_columns = receptance_weight.shape[1]
    float32 = lambda *shape: jax.ShapeDtypeStruct(shape, jnp.float32)
    bfloat16 = lambda *shape: jax.ShapeDtypeStruct(shape, jnp.bfloat16)
    both = local_call(
        stack_kernel,
        jax.ShapeDtypeStruct((2 * sequences, own_columns), tokens.dtype),
        1,
        [pltpu.SemaphoreType.DMA((2,))],
        scalars=1,
        left=2,
    )(at, tokens, previous)
    both = local_call(
        gate_kernel,
        bfloat16(*both.shape),
        1,
        cost=pl.CostEstimate(flops=40_000_000_000, transcendentals=0, bytes_accessed=200_000_000),
    )(both)
    row_pieces = gathered(both)

    vector = lambda value: value[None, :]
    needed = (
        vector(first_norm_gain),
        token_shift_share,
        receptance_weight,
        key_weight,
        value_weight,
        decay_down_map,
        decay_up_map,
        vector(decay_offset),
        strength_down_map,
        strength_up_map,
        vector(removal_key_scale),
        vector(key_damping),
        self_term_weight,
        vector(head_norm_gain),
    )
    flat_state = state.reshape(sequences, head_columns, state.shape[3])
    experts = expert_gate_weight.shape[0] * lax.axis_size("ep")
    slots = CAPACITY * experts
    dispatch, combine, down_1, down_2, down_3 = local_call(
        route_kernel,
        [bfloat16(slots, sequences), bfloat16(2 * sequences, slots)]
        + [bfloat16(expert_down_weight.shape[1], own_columns)] * 3,
        4,
        [
            pltpu.VMEM(routes.shape[::-1], routes.dtype),
            pltpu.VMEM(routes.shape[::-1], jnp.float32),
            pltpu.SemaphoreType.DMA((5,)),
        ],
        scalars=1,
        left=3,
    )(at, routes.T, chosen_expert_weight.T, expert_down_weight[0])

    down_pieces = scattered([None, down_1, down_2, down_3])[1:]
    dispatch, combine, *row_pieces = lax.optimization_barrier((dispatch, combine, *row_pieces))
    *head_terms, decay, along, value, removed, blended = local_call(
        attention_kernel,
        [bfloat16(sequences, own_columns)] * 4
        + [float32(sequences * state.shape[1], 128)]
        + [float32(sequences, head_columns)] * 2
        + [float32(sequences * state.shape[1], 128)] * 2,
        16,
        [
            pltpu.VMEM((8 * sequences, 128), jnp.float32),
            pltpu.VMEM((2, 8 * sequences, 128), jnp.float32),
        ],
        scalars=1,
    )(at, *row_pieces, *needed, output_weight, flat_state)
    arrived = scattered(head_terms)
    down_pieces = scattered([None, down_1, down_2, down_3])[1:]
    residual = tokens.astype(jnp.float32) + sum(a.astype(jnp.float32) for a in arrived)

    blocks = (2 * experts, 3 * own_columns // 2)
    outgoing, residual = local_call(
        dispatch_kernel, [bfloat16(*blocks), float32(sequences, own_columns)], 4
    )(dispatch, both, *arrived)
    exchanged = lambda value: lax.all_to_all(
        value.reshape(2, experts, -1), "ep", split_axis=1, concat_axis=1, tiled=True
    ).reshape(value.shape)
    came = exchanged(outgoing)
    came, decay, removed, blended, along, value = lax.optimization_barrier(
        (came, decay, removed, blended, along, value)
    )
    row_pieces = gathered(came)
    new_state = pl.pallas_call(
        renew_kernel,
        out_shape=float32(*flat_state.shape),
        in_specs=[pl.BlockSpec(memory_space=pltpu.VMEM)] * 5
        + [pl.BlockSpec(memory_space=pltpu.HBM)],
        out_specs=pl.BlockSpec(memory_space=pltpu.HBM),
        scratch_shapes=[
            pltpu.VMEM(flat_state.shape, jnp.float32),
            pltpu.VMEM(flat_state.shape, jnp.float32),
            pltpu.SemaphoreType.DMA((2, 8)),
        ],
        compiler_params=pltpu.CompilerParams(vmem_limit_bytes=12 * MIB),
        name="renew",
    )(decay, removed, blended, along, value, pltpu.with_memory_space_constraint(flat_state, pltpu.HBM))
    new_state, row_pieces[1] = lax.optimization_barrier((new_state, row_pieces[1]))
    new_state = new_state.reshape(state.shape)
    hidden_columns = expert_gate_weight.shape[2]
    expert_weights = (vector(second_norm_gain), expert_gate_weight[0], expert_up_weight[0])
    early = local_call(
        early_kernel, [float32(slots, hidden_columns)] * 2 + [float32(slots, 128)], 12, scalars=1
    )(at, row_pieces[0], row_pieces[2], row_pieces[3], *expert_weights)
    activation = local_call(
        hidden_kernel, bfloat16(slots, hidden_columns), 12, scalars=1
    )(at, row_pieces[1], *early, *expert_weights)
    act_pieces = scattered([activation] * 4)
    shares = local_call(
        down_kernel, bfloat16(*blocks), 8, scalars=1
    )(at, *act_pieces, *down_pieces, expert_down_weight[0])
    layer_out = local_call(
        finish_kernel, bfloat16(sequences, own_columns), 4
    )(combine, exchanged(shares), residual)
    return (layer_out, new_state)


def solution(mesh):
    in_specs = (
        P("ep", "tp"),
        P("ep", "tp"),
        P(),
        P(),
        P(None, "tp"),
        P(None, "tp"),
        P(None, "tp"),
        P(),
        P(),
        P("tp"),
        P(),
        P(),
        P("tp"),
        P("tp"),
        P("tp", None),
        P("tp"),
        P("tp", None),
        P("ep", "tp", None, None),
        P(),
        P("ep", None),
        P("ep", None),
        P("ep", None, "tp"),
        P("ep", None, "tp"),
        P("ep", "tp", None),
    )
    out_specs = (P("ep", "tp"), P("ep", "tp", None, None))

    return jax.shard_map(shards, mesh=mesh, in_specs=in_specs, out_specs=out_specs, check_vma=False)
```
